256 devices in a mesh: rep: 2 (over z_hi), fs: 16 (over z_lo, x), tp: 8 (over y, core).
Axes of the slice: x: 4, y: 4, z: 8 (z_hi: 2, z_lo: 4; z = z_hi * 4 + z_lo), core: 2. Of those that a mesh axis runs over, the one named last changes fastest.
Arguments:
- tokens: bfloat16 [32, 1024, 2048], P(('rep', 'fs')), may hold values from -6 to 6
- mix_gain: bfloat16 [2048], replicated, may hold values from 0.099609375 to 1.8984375
- value_weight: bfloat16 [2048, 1024], P('fs', 'tp'), may hold values from -0.125 to 0.125
- gate_weight: bfloat16 [2048, 1024], P('fs', 'tp'), may hold values from -0.125 to 0.125
- mix_taps: bfloat16 [31, 1024], P(None, 'tp'), may hold values from -1 to 1
- head_gain: bfloat16 [1024], P('tp'), may hold values from 0.099609375 to 1.8984375
- out_weight: bfloat16 [1024, 2048], P('fs', 'tp'), may hold values from -0.1875 to 0.1875
- ffn_gain: bfloat16 [2048], replicated, may hold values from 0.099609375 to 1.8984375
- ffgate_weight: bfloat16 [2048, 6144], P('fs', 'tp'), may hold values from -0.125 to 0.125
- up_weight: bfloat16 [2048, 6144], P('fs', 'tp'), may hold values from -0.125 to 0.125
- ff_taps: bfloat16 [3, 6144], P(None, 'tp'), may hold values from -3.5 to 3.5
- down_weight: bfloat16 [2048, 6144], P('fs', 'tp'), may hold values from -0.078125 to 0.078125
Outputs:
- layer_out: bfloat16 [32, 1024, 2048], P(('rep', 'fs'), 'tp')
The draws below stay inside these ranges and needn't reach their ends.
All inputs are finite; a program needn't handle non-finite values.
Results may differ from the reference program's by a relative error of at most 0.01.
Values may be sent and summed in bfloat16 or wider, within the bound.
A program may use at most 64 MiB of HBM per device.

```python
import jax
import jax.numpy as jnp
from jax import lax

D = 2048
CW = 1024
FF = 6144
HEAD = 128
KW = 31
KF = 3
LEN = 1024
BATCH = 32


def steps_of(stream_key, shape, cuts, smallest, largest):
    level = 1.0
    for dim, parts in cuts:
        draws = jax.random.uniform(jax.random.fold_in(jax.random.fold_in(stream_key, 6), dim), (parts,), jnp.float32, smallest / len(cuts), largest / len(cuts))
        level = level * jnp.repeat(jnp.exp(draws), shape[dim] // parts).reshape((-1,) + (1,) * (len(shape) - 1 - dim))
    return level


def normal_values(stream_key, shape, scale, bound, pieces=(), kind=jnp.bfloat16):
    level = steps_of(stream_key, shape, pieces, -0.22, 0.18) if pieces else 1.0
    array = jax.random.normal(stream_key, shape, jnp.float32) * scale * level
    return jnp.minimum(jnp.maximum(array, -bound), bound).astype(kind)


def setup_inputs(seed: int = 0) -> dict:
    key_of = jax.random.split(jax.random.key(seed), 13)
    tokens = normal_values(key_of[0], (BATCH, LEN, D), 1.0, 6.0, ((0, 32),))
    mix_gain = jnp.clip(1.0 + 0.18 * jax.random.normal(key_of[1], (D,), jnp.float32), 0.099609375, 1.8984375).astype(jnp.bfloat16)
    value_weight = normal_values(key_of[2], (D, CW), D ** -0.5, 0.125, ((0, 16), (1, 8)))
    gate_weight = normal_values(key_of[3], (D, CW), D ** -0.5, 0.125, ((0, 16), (1, 8)))
    mix_taps = normal_values(key_of[4], (KW, CW), KW ** -0.5, 1.0, ((1, 8),))
    head_gain = jnp.clip(1.0 + 0.18 * jax.random.normal(key_of[5], (CW,), jnp.float32), 0.099609375, 1.8984375).astype(jnp.bfloat16)
    out_weight = normal_values(key_of[6], (CW, D), CW ** -0.5, 0.1875, ((0, 16), (1, 8)))
    ffn_gain = jnp.clip(1.0 + 0.18 * jax.random.normal(key_of[7], (D,), jnp.float32), 0.099609375, 1.8984375).astype(jnp.bfloat16)
    ffgate_weight = normal_values(key_of[8], (D, FF), D ** -0.5, 0.125, ((0, 16), (1, 8)))
    up_weight = normal_values(key_of[9], (D, FF), D ** -0.5, 0.125, ((0, 16), (1, 8)))
    ff_taps = normal_values(key_of[10], (KF, FF), KF ** -0.5, 3.5, ((1, 8),))
    down_weight = normal_values(key_of[11], (D, FF), FF ** -0.5, 0.078125, ((0, 16), (1, 8)))
    return {"tokens": tokens, "mix_gain": mix_gain, "value_weight": value_weight, "gate_weight": gate_weight, "mix_taps": mix_taps, "head_gain": head_gain, "out_weight": out_weight, "ffn_gain": ffn_gain, "ffgate_weight": ffgate_weight, "up_weight": up_weight, "ff_taps": ff_taps, "down_weight": down_weight}


norm_floor = 0.01

def row_norm(floats_in, scales):
    floats = floats_in.astype(jnp.float32)
    scaled = floats * lax.rsqrt(lax.optimization_barrier(jnp.mean(floats * floats, axis=-1, keepdims=True)) + norm_floor)
    return (scaled * scales.astype(jnp.float32)).astype(jnp.bfloat16)

def causal_conv(signal, kernel_taps):
    reach = kernel_taps.shape[0]
    length = signal.shape[0]
    padded = jnp.pad(signal, ((reach - 1, 0), (0, 0)))
    summed = padded[0:length] * kernel_taps[0]
    for offset in range(1, reach):
        summed = summed + padded[offset:offset + length] * kernel_taps[offset]
    return summed

def head_norm(signal, scales):
    length = signal.shape[0]
    grouped = signal.reshape(length, signal.shape[1] // HEAD, HEAD)
    centre = grouped - lax.optimization_barrier(jnp.mean(grouped, axis=-1, keepdims=True))
    spread = lax.optimization_barrier(jnp.mean(centre * centre, axis=-1, keepdims=True))
    normal = (centre * lax.rsqrt(spread + norm_floor)).reshape(signal.shape)
    return normal * scales.astype(jnp.float32)

def reference(tokens, mix_gain, value_weight, gate_weight, mix_taps, head_gain, out_weight, ffn_gain, ffgate_weight, up_weight, ff_taps, down_weight):

    def sublayers(sequence):
        normed = row_norm(sequence, mix_gain)
        values = jnp.dot(normed, value_weight, preferred_element_type=jnp.float32)
        gating = jnp.dot(normed, gate_weight, preferred_element_type=jnp.float32)
        glu_out = values * jax.nn.sigmoid(gating)
        mixed_pos = causal_conv(glu_out, mix_taps.astype(jnp.float32))
        head_out = jax.nn.silu(head_norm(mixed_pos, head_gain)).astype(jnp.bfloat16)
        hidden = (sequence.astype(jnp.float32) + jnp.dot(head_out, out_weight, preferred_element_type=jnp.float32)).astype(jnp.bfloat16)
        normed_ffn = row_norm(hidden, ffn_gain)
        ffgate = jnp.dot(normed_ffn, ffgate_weight, preferred_element_type=jnp.float32)
        ff_up = jnp.dot(normed_ffn, up_weight, preferred_element_type=jnp.float32)
        product = (jax.nn.silu(causal_conv(ffgate, ff_taps.astype(jnp.float32))) * ff_up).astype(jnp.bfloat16)
        down_sum = lax.dot_general(product, down_weight, (((1,), (1,)), ((), ())), preferred_element_type=jnp.float32)
        return (hidden.astype(jnp.float32) + down_sum).astype(jnp.bfloat16)
    return lax.map(sublayers, tokens)
```

```python
import jax
import jax.numpy as jnp
from jax import lax
from jax.experimental import pallas as pl
from jax.experimental.pallas import tpu as pltpu
from jax.sharding import PartitionSpec as P

FLOOR = 0.01
CHUNKS = 4
SIDE = 4
F32 = jnp.float32
BF16 = jnp.bfloat16
NT = (((1,), (1,)), ((), ()))


class Exchange:
    def __init__(self, send_sems, recv_sems):
        self.send_sems, self.recv_sems, self.copies = send_sems, recv_sems, {}

    def send(self, key, src, dst, device):
        at = len(self.copies)
        copy = pltpu.make_async_remote_copy(
            src_ref=src,
            dst_ref=dst,
            send_sem=self.send_sems.at[at],
            recv_sem=self.recv_sems.at[at],
            device_id=device,
            device_id_type=pl.DeviceIdType.MESH,
        )
        copy.start()
        self.copies[key] = copy

    def got(self, key):
        self.copies[key].wait_recv()

    def drain(self):
        for copy in self.copies.values():
            copy.wait_send()


def kernel(
    tok_hbm, mixg, value_hbm, gate_hbm, taps, headg, out_hbm, ffng,
    fg_hbm, fu_hbm, fftaps, down_hbm,
    out_ref,
    tok, nb, vbuf, gbuf, obuf, fgbuf, fubuf, dbuf,
    tapf, fftapf, glu, heads, hid, ffg, act, prod,
    ts2, tsp, tsm, tf, r1p, r1m, r2p, r2m, xsend, xrecv, own, outf,
    send_sems, recv_sems, local_sems,
):
    length = nb.shape[0]
    rows = length // CHUNKS
    model = nb.shape[1]
    width = heads.shape[1] // 8
    cols = hid.shape[1] // 8
    units = ffg.shape[1]
    step = 256

    rep, fs, tp = lax.axis_index("rep"), lax.axis_index("fs"), lax.axis_index("tp")
    z, x = lax.div(fs, SIDE), lax.rem(fs, SIDE)
    y, core = lax.div(tp, 2), lax.rem(tp, 2)

    def around(i, d):
        return lax.rem(i + d + SIDE, SIDE)

    def along_x(d):
        return (rep, z * SIDE + around(x, d), tp)

    def along_z(d):
        at = lax.rem(rep * SIDE + z + d + 2 * SIDE, 2 * SIDE)
        return (lax.div(at, SIDE), lax.rem(at, SIDE) * SIDE + x, tp)

    def along_y(d):
        return (rep, fs, around(y, d) * 2 + core)

    partner = (rep, fs, y * 2 + 1 - core)
    yp, ym = along_y(1), along_y(-1)
    x_ring, z_ring = (along_x(1), along_x(-1)), (along_z(1), along_z(-1))
    first_ring, second_ring = (x_ring, z_ring), (z_ring, x_ring)
    place = (z, x)

    local = {}

    def load(key, src, dst):
        copy = pltpu.make_async_copy(src, dst, local_sems.at[len(local)])
        copy.start()
        local[key] = copy

    load("v", value_hbm, vbuf.at[z, x])
    load("g", gate_hbm, gbuf.at[z, x])
    half_o, half_f = out_hbm.shape[0] // 2, fg_hbm.shape[0] // 2
    quarter = down_hbm.shape[0] // 4
    for c in range(CHUNKS):
        load(("tok", c), tok_hbm.at[0, pl.ds(c * rows, rows)], tok.at[pl.ds(c * rows, rows)])
        if c == 0:
            for u in range(2):
                load(("o", u), out_hbm.at[pl.ds(u * half_o, half_o)], obuf.at[z, x, u])
    for u in range(2):
        load(("G", u), fg_hbm.at[pl.ds(u * half_f, half_f)], fgbuf.at[z, x, u])
        load(("U", u), fu_hbm.at[pl.ds(u * half_f, half_f)], fubuf.at[z, x, u])
        mine = pl.multiple_of(u * half_f + core * quarter, quarter)
        load(("D", u), down_hbm.at[pl.ds(mine, quarter)], dbuf.at[u, z, x, core])

    barrier = pltpu.get_barrier_semaphore()
    peers = (*x_ring, *z_ring, yp, ym, partner)
    for peer in peers:
        pl.semaphore_signal(barrier, inc=1, device_id=peer, device_id_type=pl.DeviceIdType.MESH)

    tapf[pl.ds(0, taps.shape[0])] = taps[...].astype(F32)
    fftapf[pl.ds(0, fftaps.shape[0])] = fftaps[...].astype(F32)
    glu[pl.ds(0, 32)] = jnp.zeros((32, glu.shape[1]), F32)
    ffg[pl.ds(0, 8)] = jnp.zeros((8, units), F32)

    pl.semaphore_wait(barrier, len(peers))
    net = Exchange(send_sems, recv_sems)

    def pick_v(u, zi, xi, h=None):
        ref = (vbuf, gbuf)[u]
        half = value_hbm.shape[0] // 2
        return ref.at[zi, xi] if h is None else ref.at[zi, xi, pl.ds(h * half, half)]

    def pick_of(ref):
        def pick(u, zi, xi, h=None):
            half = ref.shape[3] // 2
            return ref.at[zi, xi, u] if h is None else ref.at[zi, xi, u, pl.ds(h * half, half)]

        return pick

    def pick_d(u, zi, xi, h=None):
        return dbuf.at[u, zi, xi] if h is None else dbuf.at[u, zi, xi, h]

    picks = {"V": pick_v, "O": pick_of(obuf), "G": pick_of(fgbuf), "U": pick_of(fubuf), "D": pick_d}

    def near(n, u, d, h=None):
        if u == 0:
            return picks[n](0, z, around(x, d), h)
        return picks[n](1, around(z, d), x, h)

    def block(n, u, d, h):
        pair = pl.ds(2 * h, 2)
        if u == 0:
            return picks[n](0, around(z, d), pair)
        return picks[n](1, pair, around(x, d))

    def relay(key, ref, device):
        net.send(key, ref, ref, device)

    def s1(n):
        for u in range(2):
            ref = picks[n](u, z, x)
            relay((n, u, 1, "p"), ref, first_ring[u][0])
            relay((n, u, 1, "m"), ref, first_ring[u][1])

    def s2(n):
        for u in range(2):
            net.got((n, u, 1, "p"))
            relay((n, u, 2, "p"), near(n, u, -1, 0), first_ring[u][0])
            net.got((n, u, 1, "m"))
            relay((n, u, 2, "m"), near(n, u, 1, 1), first_ring[u][1])

    def s3(n):
        for u in range(2):
            net.got((n, u, 2, "p"))
            net.got((n, u, 2, "m"))
            plus, minus = second_ring[u]
            relay((n, u, 3, "p0"), block(n, u, 0, 0), plus)
            relay((n, u, 3, "m0"), block(n, u, 0, 1), minus)
            relay((n, u, 3, "p1"), block(n, u, 0, 1), plus)
            relay((n, u, 3, "m1"), block(n, u, 0, 0), minus)

    def s4(n):
        for u in range(2):
            plus, minus = second_ring[u]
            net.got((n, u, 3, "p0"))
            relay((n, u, 4, "p"), block(n, u, -1, 0), plus)
            net.got((n, u, 3, "m0"))
            relay((n, u, 4, "m"), block(n, u, 1, 1), minus)

    def s5(n):
        for u in range(2):
            net.got((n, u, 3, "p1"))
            net.got((n, u, 3, "m1"))

    def s6(n):
        for u in range(2):
            net.got((n, u, 4, "p"))
            net.got((n, u, 4, "m"))

    def chunk_ref(buf, wide, c, d, other=False, h=None):
        owner = around(y, d) * 2 + (1 - core if other else core)
        count = rows if h is None else rows // 2
        start = c * rows + (0 if h is None else h * count)
        return buf.at[pl.ds(start, count), pl.ds(pl.multiple_of(owner * wide, wide), wide)]

    def a1(n, buf, wide, c):
        ref = chunk_ref(buf, wide, c, 0)
        relay((n, c, "p"), ref, yp)
        relay((n, c, "m"), ref, ym)
        relay((n, c, "c"), ref, partner)

    def a2(n, buf, wide, c):
        net.got((n, c, "p"))
        relay((n, c, "pp"), chunk_ref(buf, wide, c, -1, h=0), yp)
        relay((n, c, "cp"), chunk_ref(buf, wide, c, -1), partner)
        net.got((n, c, "m"))
        relay((n, c, "mm"), chunk_ref(buf, wide, c, 1, h=1), ym)
        relay((n, c, "cm"), chunk_ref(buf, wide, c, 1), partner)

    def a3(n, buf, wide, c):
        net.got((n, c, "pp"))
        relay((n, c, "cpp"), chunk_ref(buf, wide, c, 2, h=0), partner)
        net.got((n, c, "mm"))
        relay((n, c, "cmm"), chunk_ref(buf, wide, c, 2, h=1), partner)

    def a4(n, c):
        for k in ("c", "cp", "cm", "cpp", "cmm"):
            net.got((n, c, k))

    def norm(src, gain, c):
        few = 16

        def body(i, _):
            at = pl.ds(pl.multiple_of(c * rows + i * few, few), few)
            value = src[at].astype(F32)
            scale = lax.rsqrt(jnp.mean(value * value, axis=-1, keepdims=True) + FLOOR)
            nb[at] = (value * scale * gain[...].astype(F32)).astype(BF16)
            return 0

        lax.fori_loop(0, rows // few, body, 0)

    def mix(c):
        at = pl.ds(c * rows, rows)
        both = jnp.concatenate(
            [vbuf[...].reshape(model, width), gbuf[...].reshape(model, width)], axis=1
        )
        pair = jnp.dot(nb[at], both, preferred_element_type=F32)
        glu[pl.ds(32 + c * rows, rows)] = pair[:, :width] * jax.nn.sigmoid(pair[:, width:])
        few, count = 64, taps.shape[0]
        lead = 32 - (count - 1)

        def body(i, _):
            base = pl.multiple_of(c * rows + i * few, few)
            total = None
            for r in range(8):
                part = None
                tall = few if r == 0 else few + 8
                for q in range(5):
                    k = 8 * q + r - lead
                    if 0 <= k < count:
                        term = glu[pl.ds(base + 8 * q, tall)] * tapf[pl.ds(k, 1)]
                        part = term if part is None else part + term
                part = part[r : r + few]
                total = part if total is None else total + part
            centre = total - jnp.mean(total, axis=-1, keepdims=True)
            spread = jnp.mean(centre * centre, axis=-1, keepdims=True)
            normal = centre * lax.rsqrt(spread + FLOOR) * headg[...].astype(F32)
            lanes = pl.ds(pl.multiple_of(tp * width, width), width)
            heads[pl.ds(base, few), lanes] = jax.nn.silu(normal).astype(BF16)
            return 0

        lax.fori_loop(0, rows // few, body, 0)

    def hidden(c):
        at = pl.ds(c * rows, rows)
        lanes = pl.ds(pl.multiple_of(tp * cols, cols), cols)
        weight = obuf[...].reshape(heads.shape[1], cols)
        total = jnp.dot(heads[at], weight, preferred_element_type=F32)
        hid[at, lanes] = (tok[at, lanes].astype(F32) + total).astype(BF16)

    def gate(c):
        at = pl.ds(c * rows, rows)

        def body(n, _):
            lanes = pl.ds(pl.multiple_of(n * step, step), step)
            weight = fgbuf[:, :, :, :, lanes].reshape(model, step)
            ffg[pl.ds(8 + c * rows, rows), lanes] = jnp.dot(
                nb[at], weight, preferred_element_type=F32
            )
            few = 32

            def conv(i, _):
                base = pl.multiple_of(c * rows + i * few, few)
                seen = ffg[pl.ds(base, few + 8), lanes]
                total = seen[6 : 6 + few] * fftapf[pl.ds(0, 1), lanes]
                total = total + seen[7 : 7 + few] * fftapf[pl.ds(1, 1), lanes]
                total = total + seen[8 : 8 + few] * fftapf[pl.ds(2, 1), lanes]
                act[pl.ds(base, few), lanes] = jax.nn.silu(total)
                return 0

            lax.fori_loop(0, rows // few, conv, 0)
            return 0

        lax.fori_loop(0, units // step, body, 0)

    def up(c):
        at = pl.ds(c * rows, rows)

        def body(n, _):
            lanes = pl.ds(pl.multiple_of(n * step, step), step)
            weight = fubuf[:, :, :, :, lanes].reshape(model, step)
            wide = jnp.dot(nb[at], weight, preferred_element_type=F32)
            prod[core, at, lanes] = (act[at, lanes] * wide).astype(BF16)
            return 0

        lax.fori_loop(0, units // step, body, 0)
        ref = prod.at[core, at]
        relay(("prod", c), ref, partner)

    offsets = (0, -1, 1, 2)
    half = rows // 2

    def down(b, d):
        zb, xb = around(z, offsets[b]), around(x, offsets[b])
        at = pl.ds(pl.multiple_of(around(y, d) * rows, rows), rows)
        total = None
        for k in range(2):
            weight = jnp.concatenate(
                [
                    dbuf[0, zb, :, k].reshape(SIDE * quarter, units),
                    dbuf[1, :, xb, k].reshape(SIDE * quarter, units),
                ],
                axis=0,
            )
            part = lax.dot_general(prod[k, at], weight, NT, preferred_element_type=F32)
            total = part if total is None else total + part
        return total

    def r1(b):
        ts2[b] = down(b, 2).astype(BF16)
        net.send(("r1", b, "p"), ts2.at[b, pl.ds(0, half)], r1p.at[b], yp)
        net.send(("r1", b, "m"), ts2.at[b, pl.ds(half, half)], r1m.at[b], ym)
        tf[0] = down(b, 1)
        tf[1] = down(b, -1)

    def r2(b):
        top, low = pl.ds(0, half), pl.ds(half, half)
        net.got(("r1", b, "p"))
        tsp[b, top] = (tf[0, top] + r1p[b].astype(F32)).astype(BF16)
        tsp[b, low] = tf[0, low].astype(BF16)
        net.send(("r2", b, "p"), tsp.at[b], r2p.at[b], yp)
        net.got(("r1", b, "m"))
        tsm[b, low] = (tf[1, low] + r1m[b].astype(F32)).astype(BF16)
        tsm[b, top] = tf[1, top].astype(BF16)
        net.send(("r2", b, "m"), tsm.at[b], r2m.at[b], ym)
        tf[2] = down(b, 0)

    def r3(b):
        net.got(("r2", b, "p"))
        net.got(("r2", b, "m"))
        mine = pl.ds(pl.multiple_of(core * half, half), half)
        other = pl.ds(pl.multiple_of((1 - core) * half, half), half)
        xsend[b] = tf[2, other] + r2p[b, other].astype(F32) + r2m[b, other].astype(F32)
        net.send(("r3", b), xsend.at[b], xrecv.at[b], partner)
        own[b] = tf[2, mine] + r2p[b, mine].astype(F32) + r2m[b, mine].astype(F32)

    def r4(b):
        zb, xb = around(z, offsets[b]), around(x, offsets[b])
        net.got(("r3", b))
        mine, other = own[b], xrecv[b]
        low = jnp.where(core == 0, mine, other)
        high = jnp.where(core == 0, other, mine)
        for j in range(SIDE):
            for u in range(2):
                at = (u * SIDE + j) * quarter
                both = jnp.concatenate([low[:, at : at + quarter], high[:, at : at + quarter]], axis=1)
                if u == 0:
                    outf[zb, j, :, pl.ds(0, 2 * quarter)] = both
                else:
                    outf[j, xb, :, pl.ds(2 * quarter, 2 * quarter)] = both

    H = ("H", heads, width)
    I = ("I", hid, cols)

    local["v"].wait()
    local["g"].wait()
    s1("V")
    for u in range(2):
        local[("o", u)].wait()
    s1("O")
    for u in range(2):
        theirs = pl.multiple_of(u * half_f + (1 - core) * quarter, quarter)
        net.send(("d", u), down_hbm.at[pl.ds(theirs, quarter)], dbuf.at[u, z, x, core], partner)
    local[("tok", 0)].wait()
    norm(tok, mixg, 0)
    s2("V")
    local[("tok", 1)].wait()
    norm(tok, mixg, 1)
    s2("O")
    s3("V")
    local[("tok", 2)].wait()
    norm(tok, mixg, 2)
    for u in range(2):
        local[("G", u)].wait()
    s1("G")
    s3("O")
    local[("tok", 3)].wait()
    norm(tok, mixg, 3)
    s4("V")
    s2("G")
    s5("V")
    s6("V")
    mix(0)
    a1(*H, 0)
    s4("O")
    s3("G")
    mix(1)
    a1(*H, 1)
    a2(*H, 0)
    for u in range(2):
        local[("U", u)].wait()
    s1("U")
    mix(2)
    a1(*H, 2)
    a2(*H, 1)
    a3(*H, 0)
    s5("O")
    s6("O")
    mix(3)
    a1(*H, 3)
    a2(*H, 2)
    a3(*H, 1)
    a4("H", 0)
    hidden(0)
    a1(*I, 0)
    a2(*H, 3)
    a3(*H, 2)
    a4("H", 1)
    s4("G")
    hidden(1)
    a1(*I, 1)
    a2(*I, 0)
    s2("U")
    a3(*H, 3)
    a4("H", 2)
    hidden(2)
    a1(*I, 2)
    a2(*I, 1)
    a3(*I, 0)
    s3("U")
    a4("H", 3)
    hidden(3)
    a1(*I, 3)
    a2(*I, 2)
    a3(*I, 1)
    a4("I", 0)
    for u in range(2):
        local[("D", u)].wait()
        net.got(("d", u))
    s1("D")
    norm(hid, ffng, 0)
    s5("G")
    s6("G")
    gate(0)
    a2(*I, 3)
    a3(*I, 2)
    a4("I", 1)
    norm(hid, ffng, 1)
    gate(1)
    s4("U")
    s2("D")
    a3(*I, 3)
    a4("I", 2)
    norm(hid, ffng, 2)
    gate(2)
    a4("I", 3)
    norm(hid, ffng, 3)
    gate(3)
    s3("D")
    s5("U")
    s6("U")
    up(0)
    up(1)
    s4("D")
    up(2)
    up(3)
    for c in range(CHUNKS):
        net.got(("prod", c))
    r1(0)
    r2(0)
    s5("D")
    r1(1)
    r3(0)
    r2(1)
    r1(2)
    r3(1)
    r4(0)
    r2(2)
    s6("D")
    r1(3)
    r3(2)
    r4(1)
    r2(3)
    r4(2)
    r3(3)
    r4(3)
    positions = length // 8
    at = pl.ds(pl.multiple_of(tp * positions, positions), positions)
    for zi in range(SIDE):
        for xi in range(SIDE):
            lanes = pl.ds((zi * SIDE + xi) * 4 * quarter, 4 * quarter)
            total = hid[at, lanes].astype(F32) + outf[zi, xi]
            out_ref[0, :, lanes] = total.astype(BF16)
    net.drain()


def on_device(
    tokens,
    mix_gain,
    value_weight,
    gate_weight,
    mix_taps,
    head_gain,
    out_weight,
    ffn_gain,
    ffgate_weight,
    up_weight,
    ff_taps,
    down_weight,
):
    _, length, model = tokens.shape
    width, cols, units = value_weight.shape[1], out_weight.shape[1], ffgate_weight.shape[1]
    deep, deep_o, deep_d = value_weight.shape[0], out_weight.shape[0], down_weight.shape[0]
    rows, positions, part = length // CHUNKS, length // 8, 2 * deep_d
    vmem = pl.BlockSpec(memory_space=pltpu.VMEM)
    hbm = pl.BlockSpec(memory_space=pl.ANY)
    four = (SIDE, SIDE)
    copies = 256
    scratch = [
        pltpu.VMEM((length, model), BF16),
        pltpu.VMEM((length, model), BF16),
        pltpu.VMEM((*four, deep, width), BF16),
        pltpu.VMEM((*four, deep, width), BF16),
        pltpu.VMEM((*four, 2, deep_o // 2, cols), BF16),
        pltpu.VMEM((*four, 2, deep // 2, units), BF16),
        pltpu.VMEM((*four, 2, deep // 2, units), BF16),
        pltpu.VMEM((2, *four, 2, deep_d // 4, units), BF16),
        pltpu.VMEM((32, width), F32),
        pltpu.VMEM((8, units), F32),
        pltpu.VMEM((32 + length, width), F32),
        pltpu.VMEM((length, 8 * width), BF16),
        pltpu.VMEM((length, 8 * cols), BF16),
        pltpu.VMEM((8 + length, units), F32),
        pltpu.VMEM((length, units), F32),
        pltpu.VMEM((2, length, units), BF16),
        pltpu.VMEM((4, rows, part), BF16),
        pltpu.VMEM((4, rows, part), BF16),
        pltpu.VMEM((4, rows, part), BF16),
        pltpu.VMEM((3, rows, part), F32),
        pltpu.VMEM((4, rows // 2, part), BF16),
        pltpu.VMEM((4, rows // 2, part), BF16),
        pltpu.VMEM((4, rows, part), BF16),
        pltpu.VMEM((4, rows, part), BF16),
        pltpu.VMEM((4, rows // 2, part), F32),
        pltpu.VMEM((4, rows // 2, part), F32),
        pltpu.VMEM((4, rows // 2, part), F32),
        pltpu.VMEM((*four, positions, deep_d), F32),
        pltpu.SemaphoreType.DMA((copies,)),
        pltpu.SemaphoreType.DMA((copies,)),
        pltpu.SemaphoreType.DMA((16,)),
    ]
    return pl.pallas_call(
        kernel,
        out_shape=jax.ShapeDtypeStruct((1, positions, model), BF16),
        in_specs=[hbm, vmem, hbm, hbm, vmem, vmem, hbm, vmem, hbm, hbm, vmem, hbm],
        out_specs=vmem,
        scratch_shapes=scratch,
        compiler_params=pltpu.CompilerParams(
            collective_id=0, has_side_effects=True, vmem_limit_bytes=60 * 1024 * 1024
        ),
        name="layer",
    )(
        tokens,
        mix_gain.reshape(1, -1),
        value_weight,
        gate_weight,
        mix_taps,
        head_gain.reshape(1, -1),
        out_weight,
        ffn_gain.reshape(1, -1),
        ffgate_weight,
        up_weight,
        ff_taps,
        down_weight,
    )


def solution(mesh):
    placed = (
        P(("rep", "fs"), None, None),
        P(),
        P("fs", "tp"),
        P("fs", "tp"),
        P(None, "tp"),
        P("tp"),
        P("fs", "tp"),
        P(),
        P("fs", "tp"),
        P("fs", "tp"),
        P(None, "tp"),
        P("fs", "tp"),
    )
    return jax.shard_map(
        on_device,
        mesh=mesh,
        in_specs=placed,
        out_specs=P(("rep", "fs"), "tp", None),
        check_vma=False,
    )
```

```python
import jax
import jax.numpy as jnp
from jax import lax
from jax.experimental import pallas as pl
from jax.experimental.pallas import tpu as pltpu
from jax.sharding import PartitionSpec as P

FLOOR = 0.01
CHUNKS = 4
SIDE = 4
F32 = jnp.float32
BF16 = jnp.bfloat16
NT = (((1,), (1,)), ((), ()))


SETS = {"V": "x", "U": "x", "O": "y", "D": "y", "G": "z"}
RING = {"H": 1, "I": 1, "r1": 1, "r2": 1}
FAR = {"p": "pp", "m": "mm"}
POOL = 40
RECEIVES = 94


def slot_of(key):
    name = key[0]
    if name in SETS:
        return (SETS[name], *key[1:])
    if name in RING and key[2] != "c":
        return ("ring", key[1], FAR[key[2]] if name == "r2" else key[2])
    return key


class Exchange:
    def __init__(self, send_sems, recv_sems):
        self.send_sems, self.recv_sems, self.copies, self.slots = send_sems, recv_sems, {}, {}
        self.started = []

    def send(self, key, src, dst, device):
        turn = len(self.started)
        if turn >= POOL:
            self.started[turn - POOL].wait_send()
        at = self.slots.setdefault(slot_of(key), len(self.slots))
        copy = pltpu.make_async_remote_copy(
            src_ref=src,
            dst_ref=dst,
            send_sem=self.send_sems.at[turn % POOL],
            recv_sem=self.recv_sems.at[at],
            device_id=device,
            device_id_type=pl.DeviceIdType.MESH,
        )
        copy.start()
        self.started.append(copy)
        self.copies[key] = copy

    def got(self, key):
        self.copies[key].wait_recv()

    def drain(self):
        assert len(self.slots) == RECEIVES, len(self.slots)
        for copy in self.started[-POOL:]:
            copy.wait_send()


def kernel(
    tok_hbm, mixg, value_hbm, gate_hbm, taps, headg, out_hbm, ffng,
    fg_hbm, fu_hbm, fftaps, down_hbm,
    out_ref,
    tok, nb, vbuf, gbuf, obuf, fgbuf, fubuf, dbuf,
    tapf, fftapf, glu, heads, hid, ffg, act, prod,
    ts2, tsp, tsm, tf, r1p, r1m, r2p, r2m, xsend, xrecv, own, outf,
    send_sems, recv_sems, local_sems,
):
    length = nb.shape[0]
    rows = length // CHUNKS
    model = nb.shape[1]
    width = heads.shape[1] // 8
    cols = hid.shape[1] // 8
    units = ffg.shape[1]
    step = 256

    rep, fs, tp = lax.axis_index("rep"), lax.axis_index("fs"), lax.axis_index("tp")
    z, x = lax.div(fs, SIDE), lax.rem(fs, SIDE)
    y, core = lax.div(tp, 2), lax.rem(tp, 2)

    def around(i, d):
        return lax.rem(i + d + SIDE, SIDE)

    def along_x(d):
        return (rep, z * SIDE + around(x, d), tp)

    def along_z(d):
        at = lax.rem(rep * SIDE + z + d + 2 * SIDE, 2 * SIDE)
        return (lax.div(at, SIDE), lax.rem(at, SIDE) * SIDE + x, tp)

    def along_y(d):
        return (rep, fs, around(y, d) * 2 + core)

    partner = (rep, fs, y * 2 + 1 - core)
    yp, ym = along_y(1), along_y(-1)
    x_ring, z_ring = (along_x(1), along_x(-1)), (along_z(1), along_z(-1))
    first_ring, second_ring = (x_ring, z_ring), (z_ring, x_ring)
    place = (z, x)

    barrier = pltpu.get_barrier_semaphore()
    peers = (*x_ring, *z_ring, yp, ym, partner)
    for peer in peers:
        pl.semaphore_signal(barrier, inc=1, device_id=peer, device_id_type=pl.DeviceIdType.MESH)

    local = {}

    def load(key, src, dst):
        copy = pltpu.make_async_copy(src, dst, local_sems.at[len(local)])
        copy.start()
        local[key] = copy

    load("v", value_hbm, vbuf.at[z, x])
    load("g", gate_hbm, gbuf.at[z, x])
    half_o, half_f = out_hbm.shape[0] // 2, fg_hbm.shape[0] // 2
    quarter = down_hbm.shape[0] // 4
    for c in range(CHUNKS):
        load(("tok", c), tok_hbm.at[0, pl.ds(c * rows, rows)], tok.at[pl.ds(c * rows, rows)])
        if c == 0:
            for u in range(2):
                load(("O", u), out_hbm.at[pl.ds(u * half_o, half_o)], obuf.at[z, x, u])
    for u in range(2):
        load(("G", u), fg_hbm.at[pl.ds(u * half_f, half_f)], fgbuf.at[z, x, u])
        load(("U", u), fu_hbm.at[pl.ds(u * half_f, half_f)], fubuf.at[z, x, u])
        mine = pl.multiple_of(u * half_f + core * quarter, quarter)
        load(("D", u), down_hbm.at[pl.ds(mine, quarter)], dbuf.at[u, z, x, core])

    tapf[pl.ds(0, taps.shape[0])] = taps[...].astype(F32)
    fftapf[pl.ds(0, fftaps.shape[0])] = fftaps[...].astype(F32)
    glu[pl.ds(0, 32)] = jnp.zeros((32, glu.shape[1]), F32)
    ffg[pl.ds(0, 8)] = jnp.zeros((8, units), F32)

    net = Exchange(send_sems, recv_sems)

    def pick_v(u, zi, xi, h=None):
        ref = (vbuf, gbuf)[u]
        half = value_hbm.shape[0] // 2
        return ref.at[zi, xi] if h is None else ref.at[zi, xi, pl.ds(h * half, half)]

    def pick_of(ref):
        def pick(u, zi, xi, h=None):
            half = ref.shape[3] // 2
            return ref.at[zi, xi, u] if h is None else ref.at[zi, xi, u, pl.ds(h * half, half)]

        return pick

    def pick_d(u, zi, xi, h=None):
        return dbuf.at[u, zi, xi] if h is None else dbuf.at[u, zi, xi, h]

    picks = {"V": pick_v, "O": pick_of(obuf), "G": pick_of(fgbuf), "U": pick_of(fubuf), "D": pick_d}

    def near(n, u, d, h=None):
        if u == 0:
            return picks[n](0, z, around(x, d), h)
        return picks[n](1, around(z, d), x, h)

    def block(n, u, d, h):
        pair = pl.ds(2 * h, 2)
        if u == 0:
            return picks[n](0, around(z, d), pair)
        return picks[n](1, pair, around(x, d))

    def relay(key, ref, device):
        net.send(key, ref, ref, device)

    def s1(n, u):
        if u == 0 or n in "V":
            ready(*own_blocks[n])
        ref = picks[n](u, z, x)
        relay((n, u, 1, "p"), ref, first_ring[u][0])
        relay((n, u, 1, "m"), ref, first_ring[u][1])

    def s2(n, u):
        net.got((n, u, 1, "p"))
        net.got((n, u, 1, "m"))
        relay((n, u, 2, "p"), near(n, u, -1, 0), first_ring[u][0])
        relay((n, u, 2, "m"), near(n, u, 1, 1), first_ring[u][1])

    def s3(n, u):
        net.got((n, u, 2, "p"))
        net.got((n, u, 2, "m"))
        plus, minus = second_ring[u]
        relay((n, u, 3, "p0"), block(n, u, 0, 0), plus)
        relay((n, u, 3, "m0"), block(n, u, 0, 1), minus)
        relay((n, u, 3, "p1"), block(n, u, 0, 1), plus)
        relay((n, u, 3, "m1"), block(n, u, 0, 0), minus)

    def s4(n, u):
        plus, minus = second_ring[u]
        net.got((n, u, 3, "p0"))
        relay((n, u, 4, "p"), block(n, u, -1, 0), plus)
        net.got((n, u, 3, "m0"))
        relay((n, u, 4, "m"), block(n, u, 1, 1), minus)

    def s5(n, u):
        net.got((n, u, 3, "p1"))
        net.got((n, u, 3, "m1"))

    def s6(n, u):
        net.got((n, u, 4, "p"))
        net.got((n, u, 4, "m"))

    def chunk_ref(buf, wide, c, d, h=None):
        count = rows if h is None else rows // 2
        start = c * rows + (0 if h is None else h * count)
        lane = pl.multiple_of(core * SIDE * wide + around(y, d) * wide, wide)
        return buf.at[pl.ds(start, count), pl.ds(lane, wide)]

    def a1(n, buf, wide, c):
        ref = chunk_ref(buf, wide, c, 0)
        relay((n, c, "p"), ref, yp)
        relay((n, c, "m"), ref, ym)

    def a2(n, buf, wide, c):
        net.got((n, c, "p"))
        net.got((n, c, "m"))
        relay((n, c, "pp"), chunk_ref(buf, wide, c, -1, h=0), yp)
        relay((n, c, "mm"), chunk_ref(buf, wide, c, 1, h=1), ym)

    def a3(n, buf, wide, c):
        net.got((n, c, "pp"))
        net.got((n, c, "mm"))
        lane = pl.multiple_of(core * SIDE * wide, SIDE * wide)
        relay((n, c, "c"), buf.at[pl.ds(c * rows, rows), pl.ds(lane, SIDE * wide)], partner)

    def a4(n, c):
        net.got((n, c, "c"))

    def norm(src, gain, c, starts):
        few, wide = 16, model // len(starts)

        def body(i, _):
            at = pl.ds(pl.multiple_of(c * rows + i * few, few), few)
            parts = [src[at, pl.ds(start, wide)] for start in starts]
            value = jnp.concatenate(parts, axis=1).astype(F32)
            scale = lax.rsqrt(jnp.mean(value * value, axis=-1, keepdims=True) + FLOOR)
            nb[at] = (value * scale * gain[...].astype(F32).reshape(1, model)).astype(BF16)
            return 0

        lax.fori_loop(0, rows // few, body, 0, unroll=4)

    def mixa(c):
        at = pl.ds(c * rows, rows)
        both = jnp.concatenate(
            [vbuf[...].reshape(model, width), gbuf[...].reshape(model, width)], axis=1
        )
        pair = jnp.dot(nb[at], both, preferred_element_type=F32)
        glu[pl.ds(32 + c * rows, rows)] = pair[:, :width] * jax.nn.sigmoid(pair[:, width:])

    def mix(c):
        few, count = 64, taps.shape[0]
        lead = 32 - (count - 1)

        def body(i, _):
            base = pl.multiple_of(c * rows + i * few, few)
            total = None
            for r in range(8):
                part = None
                tall = few if r == 0 else few + 8
                for q in range(5):
                    k = 8 * q + r - lead
                    if 0 <= k < count:
                        term = glu[pl.ds(base + 8 * q, tall)] * tapf[pl.ds(k, 1)]
                        part = term if part is None else part + term
                part = part[r : r + few]
                total = part if total is None else total + part
            centre = total - jnp.mean(total, axis=-1, keepdims=True)
            spread = jnp.mean(centre * centre, axis=-1, keepdims=True)
            normal = centre * lax.rsqrt(spread + FLOOR) * headg[...].astype(F32)
            lanes = pl.ds(pl.multiple_of(core * SIDE * width + y * width, width), width)
            heads[pl.ds(base, few), lanes] = jax.nn.silu(normal).astype(BF16)
            return 0

        lax.fori_loop(0, rows // few, body, 0)

    def hidden(c):
        at = pl.ds(c * rows, rows)
        lanes = pl.ds(pl.multiple_of(tp * cols, cols), cols)
        mine = pl.ds(pl.multiple_of(core * SIDE * cols + y * cols, cols), cols)
        weight = jnp.concatenate(
            [obuf[:, 2 * k : 2 * k + 2].reshape(SIDE * width, cols) for k in range(2)], axis=0
        )
        total = jnp.dot(heads[at], weight, preferred_element_type=F32)
        hid[at, mine] = (tok[at, lanes].astype(F32) + total).astype(BF16)

    def gate(c, n):
        at, lanes = pl.ds(c * rows, rows), pl.ds(n * step, step)
        weight = fgbuf[:, :, :, :, lanes].reshape(model, step)
        ffg[pl.ds(8 + c * rows, rows), lanes] = jnp.dot(nb[at], weight, preferred_element_type=F32)
        few = 32
        for i in range(rows // few):
            base = c * rows + i * few
            seen = ffg[pl.ds(base, few + 8), lanes]
            total = seen[6 : 6 + few] * fftapf[pl.ds(0, 1), lanes]
            total = total + seen[7 : 7 + few] * fftapf[pl.ds(1, 1), lanes]
            total = total + seen[8 : 8 + few] * fftapf[pl.ds(2, 1), lanes]
            act[pl.ds(base, few), lanes] = jax.nn.silu(total)

    def up(d, n):
        at = pl.ds(pl.multiple_of(around(y, d) * rows, rows), rows)
        lanes = pl.ds(n * step, step)
        weight = fubuf[:, :, :, :, lanes].reshape(model, step)
        wide = jnp.dot(nb[at], weight, preferred_element_type=F32)
        prod[core, at, lanes] = (act[at, lanes] * wide).astype(BF16)
        if n == units // step - 1:
            relay(("prod", d), prod.at[core, at], partner)

    def up_in(d):
        net.got(("prod", d))

    offsets = (0, -1, 1, 2)
    half = rows // 2

    def down(b, d):
        zb, xb = around(z, offsets[b]), around(x, offsets[b])
        at = pl.ds(pl.multiple_of(around(y, d) * rows, rows), rows)
        total = None
        for k in range(2):
            weight = jnp.concatenate(
                [
                    dbuf[0, zb, :, k].reshape(SIDE * quarter, units),
                    dbuf[1, :, xb, k].reshape(SIDE * quarter, units),
                ],
                axis=0,
            )
            part = lax.dot_general(prod[k, at], weight, NT, preferred_element_type=F32)
            total = part if total is None else total + part
        return total

    def ra(b):
        ts2[b] = down(b, 2).astype(BF16)
        net.send(("r1", b, "p"), ts2.at[b, pl.ds(0, half)], r1p.at[b], yp)
        net.send(("r1", b, "m"), ts2.at[b, pl.ds(half, half)], r1m.at[b], ym)

    def rb(b):
        tf[b, 0] = down(b, 1)
        tf[b, 1] = down(b, -1)

    def rc(b):
        top, low = pl.ds(0, half), pl.ds(half, half)
        net.got(("r1", b, "p"))
        net.got(("r1", b, "m"))
        tsp[b, top] = (tf[b, 0, top] + r1p[b].astype(F32)).astype(BF16)
        tsp[b, low] = tf[b, 0, low].astype(BF16)
        net.send(("r2", b, "p"), tsp.at[b], r2p.at[b], yp)
        tsm[b, low] = (tf[b, 1, low] + r1m[b].astype(F32)).astype(BF16)
        tsm[b, top] = tf[b, 1, top].astype(BF16)
        net.send(("r2", b, "m"), tsm.at[b], r2m.at[b], ym)

    def rd(b):
        tf[b, 2] = down(b, 0)

    def re(b):
        net.got(("r2", b, "p"))
        net.got(("r2", b, "m"))
        mine = pl.ds(pl.multiple_of(core * half, half), half)
        other = pl.ds(pl.multiple_of((1 - core) * half, half), half)
        xsend[b] = tf[b, 2, other] + r2p[b, other].astype(F32) + r2m[b, other].astype(F32)
        net.send(("r3", b), xsend.at[b], xrecv.at[b], partner)
        own[b] = tf[b, 2, mine] + r2p[b, mine].astype(F32) + r2m[b, mine].astype(F32)

    def rf(b):
        zb, xb = around(z, offsets[b]), around(x, offsets[b])
        net.got(("r3", b))
        mine, other = own[b], xrecv[b]
        low = jnp.where(core == 0, mine, other)
        high = jnp.where(core == 0, other, mine)
        for j in range(SIDE):
            for u in range(2):
                at = (u * SIDE + j) * quarter
                both = jnp.concatenate([low[:, at : at + quarter], high[:, at : at + quarter]], axis=1)
                if u == 0:
                    outf[zb, j, :, pl.ds(0, 2 * quarter)] = both
                else:
                    outf[j, xb, :, pl.ds(2 * quarter, 2 * quarter)] = both

    H = ("H", heads, width)
    own_blocks = {
        "V": ("v", "g"),
        **{n: ((n, 0), (n, 1)) for n in "OGUD"},
    }
    in_order = [(t % 2) * SIDE * cols + (t // 2) * cols for t in range(8)]
    I = ("I", hid, cols)

    def ready(*keys):
        for key in keys:
            if key in local:
                local.pop(key).wait()

    def halves():
        for u in range(2):
            theirs = pl.multiple_of(u * half_f + (1 - core) * quarter, quarter)
            net.send(("d", u), down_hbm.at[pl.ds(theirs, quarter)], dbuf.at[u, z, x, core], partner)

    def halves_in():
        for u in range(2):
            net.got(("d", u))

    def normed(c):
        ready(("tok", c))
        norm(tok, mixg, c, [0])

    def renormed(c):
        norm(hid, ffng, c, in_order)

    def meet():
        pl.semaphore_wait(barrier, len(peers))

    for step_of, *given in (
        (normed, 0), (normed, 1), (meet,), (s1, "V", 0), (s1, "V", 1), (halves,), (halves_in,),
        (normed, 2), (normed, 3), (s2, "V", 0), (s2, "V", 1), (s1, "O", 0), (s1, "O", 1), (s1, "G", 0),
        (s1, "G", 1), (s3, "V", 0), (s3, "V", 1), (s2, "O", 0), (s2, "O", 1), (s2, "G", 0), (s2, "G", 1),
        (s4, "V", 0), (s4, "V", 1), (s5, "V", 0), (s5, "V", 1), (s3, "O", 0), (s3, "O", 1), (s3, "G", 0),
        (s3, "G", 1), (s6, "V", 0), (s6, "V", 1), (s1, "U", 0), (s1, "U", 1), (mixa, 0), (mix, 0),
        (a1, *H, 0), (s4, "O", 0), (s4, "O", 1), (s5, "O", 0), (s5, "O", 1), (mixa, 1), (mix, 1),
        (a1, *H, 1), (mixa, 2), (mix, 2), (a1, *H, 2), (mixa, 3), (s4, "G", 0), (s4, "G", 1), (mix, 3),
        (a2, *H, 0), (a1, *H, 3), (a2, *H, 1), (a2, *H, 2), (s5, "G", 0), (s5, "G", 1), (a3, *H, 0),
        (a2, *H, 3), (a4, "H", 0), (s2, "U", 0), (s2, "U", 1), (a3, *H, 1), (s6, "O", 0), (s6, "O", 1),
        (s1, "D", 0), (s1, "D", 1), (hidden, 0), (a3, *H, 2), (a1, *I, 0), (a4, "H", 1), (hidden, 1),
        (a1, *I, 1), (a4, "H", 2), (hidden, 2), (a3, *H, 3), (a4, "H", 3), (hidden, 3), (s6, "G", 0),
        (s6, "G", 1), (s3, "U", 0), (s3, "U", 1), (a2, *I, 0), (a1, *I, 2), (s2, "D", 0), (s2, "D", 1),
        (a2, *I, 1), (a1, *I, 3), (a3, *I, 0), (a4, "I", 0), (renormed, 0), (s4, "U", 0), (s4, "U", 1),
        (gate, 0, 0), (a2, *I, 2), (gate, 0, 1), (gate, 0, 2), (a3, *I, 1), (s5, "U", 0), (s5, "U", 1),
        (a4, "I", 1), (renormed, 1), (a2, *I, 3), (gate, 1, 0), (s3, "D", 0), (s3, "D", 1), (gate, 1, 1),
        (a3, *I, 2), (gate, 1, 2), (a4, "I", 2), (renormed, 2), (gate, 2, 0), (a3, *I, 3), (s6, "U", 0),
        (s6, "U", 1), (gate, 2, 1), (gate, 2, 2), (a4, "I", 3), (renormed, 3), (gate, 3, 0), (gate, 3, 1),
        (gate, 3, 2), (s4, "D", 0), (s4, "D", 1), (up, 2, 0), (up, 2, 1), (up, 2, 2), (up, 1, 0),
        (up, 1, 1), (up, 1, 2), (up, -1, 0), (up_in, 2), (ra, 0), (s5, "D", 0), (s5, "D", 1), (ra, 1),
        (ra, 2), (up_in, 1), (up, -1, 1), (up, -1, 2), (up, 0, 0), (up, 0, 1), (up, 0, 2), (up_in, -1),
        (rb, 0), (s6, "D", 0), (s6, "D", 1), (rc, 0), (ra, 3), (rb, 1), (up_in, 0), (rc, 1), (rd, 0),
        (rd, 1), (rb, 2), (rc, 2), (rd, 2), (rb, 3), (rd, 3), (re, 0), (rc, 3), (rf, 0), (re, 1), (rf, 1),
        (re, 2), (rf, 2), (re, 3), (rf, 3),
    ):
        tag = "_".join(str(part) for part in given if isinstance(part, (int, str)))
        with jax.named_scope(step_of.__name__ + "_" + tag):
            step_of(*given)
    positions = length // 8
    at = pl.ds(pl.multiple_of(tp * positions, positions), positions)
    with jax.named_scope("result"):
        for zi in range(SIDE):
            for xi in range(SIDE):
                lanes = pl.ds((zi * SIDE + xi) * 4 * quarter, 4 * quarter)
                start = in_order[2 * zi + xi // 2] + (xi % 2) * 4 * quarter
                total = hid[at, pl.ds(start, 4 * quarter)].astype(F32) + outf[zi, xi]
                out_ref[0, :, lanes] = total.astype(BF16)
    with jax.named_scope("drain"):
        net.drain()


def on_device(
    tokens,
    mix_gain,
    value_weight,
    gate_weight,
    mix_taps,
    head_gain,
    out_weight,
    ffn_gain,
    ffgate_weight,
    up_weight,
    ff_taps,
    down_weight,
):
    _, length, model = tokens.shape
    width, cols, units = value_weight.shape[1], out_weight.shape[1], ffgate_weight.shape[1]
    deep, deep_o, deep_d = value_weight.shape[0], out_weight.shape[0], down_weight.shape[0]
    rows, positions, part = length // CHUNKS, length // 8, 2 * deep_d
    vmem = pl.BlockSpec(memory_space=pltpu.VMEM)
    hbm = pl.BlockSpec(memory_space=pl.ANY)
    four = (SIDE, SIDE)
    scratch = [
        pltpu.VMEM((length, model), BF16),
        pltpu.VMEM((length, model), BF16),
        pltpu.VMEM((*four, deep, width), BF16),
        pltpu.VMEM((*four, deep, width), BF16),
        pltpu.VMEM((*four, 2, deep_o // 2, cols), BF16),
        pltpu.VMEM((*four, 2, deep // 2, units), BF16),
        pltpu.VMEM((*four, 2, deep // 2, units), BF16),
        pltpu.VMEM((2, *four, 2, deep_d // 4, units), BF16),
        pltpu.VMEM((32, width), F32),
        pltpu.VMEM((8, units), F32),
        pltpu.VMEM((32 + length, width), F32),
        pltpu.VMEM((length, 8 * width), BF16),
        pltpu.VMEM((length, 8 * cols), BF16),
        pltpu.VMEM((8 + length, units), F32),
        pltpu.VMEM((length, units), F32),
        pltpu.VMEM((2, length, units), BF16),
        pltpu.VMEM((4, rows, part), BF16),
        pltpu.VMEM((4, rows, part), BF16),
        pltpu.VMEM((4, rows, part), BF16),
        pltpu.VMEM((4, 3, rows, part), F32),
        pltpu.VMEM((4, rows // 2, part), BF16),
        pltpu.VMEM((4, rows // 2, part), BF16),
        pltpu.VMEM((4, rows, part), BF16),
        pltpu.VMEM((4, rows, part), BF16),
        pltpu.VMEM((4, rows // 2, part), F32),
        pltpu.VMEM((4, rows // 2, part), F32),
        pltpu.VMEM((4, rows // 2, part), F32),
        pltpu.VMEM((*four, positions, deep_d), F32),
        pltpu.SemaphoreType.DMA((POOL,)),
        pltpu.SemaphoreType.DMA((RECEIVES,)),
        pltpu.SemaphoreType.DMA((14,)),
    ]
    return pl.pallas_call(
        kernel,
        out_shape=jax.ShapeDtypeStruct((1, positions, model), BF16),
        in_specs=[hbm, vmem, hbm, hbm, vmem, vmem, hbm, vmem, hbm, hbm, vmem, hbm],
        out_specs=vmem,
        scratch_shapes=scratch,
        compiler_params=pltpu.CompilerParams(
            collective_id=0, has_side_effects=True, vmem_limit_bytes=60 * 1024 * 1024
        ),
        name="layer",
    )(
        tokens,
        mix_gain,
        value_weight,
        gate_weight,
        mix_taps,
        head_gain.reshape(1, -1),
        out_weight,
        ffn_gain,
        ffgate_weight,
        up_weight,
        ff_taps,
        down_weight,
    )


def solution(mesh):
    placed = (
        P(("rep", "fs"), None, None),
        P(),
        P("fs", "tp"),
        P("fs", "tp"),
        P(None, "tp"),
        P("tp"),
        P("fs", "tp"),
        P(),
        P("fs", "tp"),
        P("fs", "tp"),
        P(None, "tp"),
        P("fs", "tp"),
    )
    return jax.shard_map(
        on_device,
        mesh=mesh,
        in_specs=placed,
        out_specs=P(("rep", "fs"), "tp", None),
        check_vma=False,
    )
```

```python
import jax
import jax.numpy as jnp
from jax import lax
from jax.experimental import pallas as pl
from jax.experimental.pallas import tpu as pltpu
from jax.sharding import PartitionSpec as P

FLOOR = 0.01
SIZES = (192, 256, 256, 192, 128)
SIDE = 4
F32 = jnp.float32
BF16 = jnp.bfloat16
NT = (((1,), (1,)), ((), ()))


SETS = {"V": "x", "U": "x", "O": "y", "D": "y", "G": "z"}
RING = {"H": 1, "I": 1, "r1": 1, "r2": 1}
FAR = {"p": "pp", "m": "mm"}
POOL = 32
RECEIVES = 116


def slot_of(key):
    name = key[0]
    if name in SETS:
        return (SETS[name] if key[2] > 2 else name, *key[1:])
    if name in RING and key[2] != "c":
        return ("ring", key[1], FAR[key[2]] if name == "r2" else key[2])
    return key


class Exchange:
    def __init__(self, send_sems, recv_sems):
        self.send_sems, self.recv_sems, self.copies, self.slots = send_sems, recv_sems, {}, {}
        self.started = []

    def send(self, key, src, dst, device):
        turn = len(self.started)
        if turn >= POOL:
            self.started[turn - POOL].wait_send()
        at = self.slots.setdefault(slot_of(key), len(self.slots))
        copy = pltpu.make_async_remote_copy(
            src_ref=src,
            dst_ref=dst,
            send_sem=self.send_sems.at[turn % POOL],
            recv_sem=self.recv_sems.at[at],
            device_id=device,
            device_id_type=pl.DeviceIdType.MESH,
        )
        copy.start()
        self.started.append(copy)
        self.copies[key] = copy

    def got(self, key):
        self.copies[key].wait_recv()

    def drain(self):
        assert len(self.slots) == RECEIVES, len(self.slots)
        for copy in self.started[-POOL:]:
            copy.wait_send()


def kernel(
    tok_hbm, mixg, value_hbm, gate_hbm, taps, headg, out_hbm, ffng,
    fg_hbm, fu_hbm, fftaps, down_hbm,
    out_ref,
    tok, nb, vbuf, gbuf, obuf, fgbuf, fubuf, dbuf,
    tapf, fftapf, glu, heads, hid, ffg, act, prod,
    ts2, tsp, tsm, tf, r1p, r1m, r2p, r2m, xsend, xrecv, own, outf,
    send_sems, recv_sems, local_sems,
):
    length = nb.shape[0]
    rows = length // SIDE
    starts = [sum(SIZES[:c]) for c in range(len(SIZES))]
    model = nb.shape[1]
    width = heads.shape[1] // 8
    cols = hid.shape[1] // 8
    units = ffg.shape[1]
    step = 256

    rep, fs, tp = lax.axis_index("rep"), lax.axis_index("fs"), lax.axis_index("tp")
    z, x = lax.div(fs, SIDE), lax.rem(fs, SIDE)
    y, core = lax.div(tp, 2), lax.rem(tp, 2)

    def around(i, d):
        return lax.rem(i + d + SIDE, SIDE)

    def along_x(d):
        return (rep, z * SIDE + around(x, d), tp)

    def along_z(d):
        at = lax.rem(rep * SIDE + z + d + 2 * SIDE, 2 * SIDE)
        return (lax.div(at, SIDE), lax.rem(at, SIDE) * SIDE + x, tp)

    def along_y(d):
        return (rep, fs, around(y, d) * 2 + core)

    partner = (rep, fs, y * 2 + 1 - core)
    yp, ym = along_y(1), along_y(-1)
    x_ring, z_ring = (along_x(1), along_x(-1)), (along_z(1), along_z(-1))
    first_ring, second_ring = (x_ring, z_ring), (z_ring, x_ring)
    place = (z, x)

    barrier = pltpu.get_barrier_semaphore()
    peers = (*x_ring, *z_ring, yp, ym, partner)
    for peer in peers:
        pl.semaphore_signal(barrier, inc=1, device_id=peer, device_id_type=pl.DeviceIdType.MESH)

    local = {}

    def load(key, src, dst):
        copy = pltpu.make_async_copy(src, dst, local_sems.at[len(local)])
        copy.start()
        local[key] = copy

    load("v", value_hbm, vbuf.at[z, x])
    load("g", gate_hbm, gbuf.at[z, x])
    half_o, half_f = out_hbm.shape[0] // 2, fg_hbm.shape[0] // 2
    quarter = down_hbm.shape[0] // 4
    net = Exchange(send_sems, recv_sems)

    def pick_v(u, zi, xi, h=None):
        ref = (vbuf, gbuf)[u]
        half = value_hbm.shape[0] // 2
        return ref.at[zi, xi] if h is None else ref.at[zi, xi, pl.ds(h * half, half)]

    def pick_of(ref):
        def pick(u, zi, xi, h=None):
            half = ref.shape[3] // 2
            return ref.at[zi, xi, u] if h is None else ref.at[zi, xi, u, pl.ds(h * half, half)]

        return pick

    def pick_d(u, zi, xi, h=None):
        return dbuf.at[u, zi, xi] if h is None else dbuf.at[u, zi, xi, h]

    picks = {"V": pick_v, "O": pick_of(obuf), "G": pick_of(fgbuf), "U": pick_of(fubuf), "D": pick_d}

    def near(n, u, d, h=None):
        if u == 0:
            return picks[n](0, z, around(x, d), h)
        return picks[n](1, around(z, d), x, h)

    def block(n, u, d, h):
        pair = pl.ds(2 * h, 2)
        if u == 0:
            return picks[n](0, around(z, d), pair)
        return picks[n](1, pair, around(x, d))

    def relay(key, ref, device):
        net.send(key, ref, ref, device)

    def s1(n, u):
        if u == 0 or n in "V":
            ready(*own_blocks[n])
        ref = picks[n](u, z, x)
        relay((n, u, 1, "p"), ref, first_ring[u][0])
        relay((n, u, 1, "m"), ref, first_ring[u][1])

    def s2(n, u):
        net.got((n, u, 1, "p"))
        net.got((n, u, 1, "m"))
        relay((n, u, 2, "p"), near(n, u, -1, 0), first_ring[u][0])
        relay((n, u, 2, "m"), near(n, u, 1, 1), first_ring[u][1])

    def s3(n, u):
        for v in {"U": (0, 1), "D": (0, 1)}.get(n, (u,)) if u == 0 or n not in "UD" else ():
            net.got((n, v, 2, "p"))
            net.got((n, v, 2, "m"))
        plus, minus = second_ring[u]
        relay((n, u, 3, "p0"), block(n, u, 0, 0), plus)
        relay((n, u, 3, "m0"), block(n, u, 0, 1), minus)
        relay((n, u, 3, "p1"), block(n, u, 0, 1), plus)
        relay((n, u, 3, "m1"), block(n, u, 0, 0), minus)

    def s4(n, u):
        plus, minus = second_ring[u]
        net.got((n, u, 3, "p0"))
        relay((n, u, 4, "p"), block(n, u, -1, 0), plus)
        net.got((n, u, 3, "m0"))
        relay((n, u, 4, "m"), block(n, u, 1, 1), minus)

    def s5(n, u):
        net.got((n, u, 3, "p1"))
        net.got((n, u, 3, "m1"))

    def s6(n, u):
        net.got((n, u, 4, "p"))
        net.got((n, u, 4, "m"))

    def chunk_ref(buf, wide, c, d, h=None):
        count = SIZES[c] if h is None else SIZES[c] // 2
        start = starts[c] + (0 if h is None else h * count)
        lane = pl.multiple_of(core * SIDE * wide + around(y, d) * wide, wide)
        return buf.at[pl.ds(start, count), pl.ds(lane, wide)]

    def a1(n, buf, wide, c):
        ref = chunk_ref(buf, wide, c, 0)
        relay((n, c, "p"), ref, yp)
        relay((n, c, "m"), ref, ym)

    def a2(n, buf, wide, c):
        net.got((n, c, "p"))
        net.got((n, c, "m"))
        relay((n, c, "pp"), chunk_ref(buf, wide, c, -1, h=0), yp)
        relay((n, c, "mm"), chunk_ref(buf, wide, c, 1, h=1), ym)

    def a3(n, buf, wide, c):
        net.got((n, c, "pp"))
        net.got((n, c, "mm"))
        lane = pl.multiple_of(core * SIDE * wide, SIDE * wide)
        relay((n, c, "c"), buf.at[pl.ds(starts[c], SIZES[c]), pl.ds(lane, SIDE * wide)], partner)

    def a4(n, c):
        net.got((n, c, "c"))

    def norm(src, gain, first, count, lanes):
        few, wide = 16, model // len(lanes)

        def body(i, _):
            at = pl.ds(pl.multiple_of(first + i * few, few), few)
            parts = [src[at, pl.ds(start, wide)] for start in lanes]
            value = jnp.concatenate(parts, axis=1).astype(F32)
            scale = lax.rsqrt(jnp.mean(value * value, axis=-1, keepdims=True) + FLOOR)
            nb[at] = (value * scale * gain[...].astype(F32).reshape(1, model)).astype(BF16)
            return 0

        lax.fori_loop(0, count // few, body, 0, unroll=4)

    def mixa(c):
        at = pl.ds(starts[c], SIZES[c])
        both = jnp.concatenate(
            [vbuf[...].reshape(model, width), gbuf[...].reshape(model, width)], axis=1
        )
        pair = jnp.dot(nb[at], both, preferred_element_type=F32)
        glu[pl.ds(32 + starts[c], SIZES[c])] = pair[:, :width] * jax.nn.sigmoid(pair[:, width:])

    def mix(c):
        few, count = 64, taps.shape[0]
        lead = 32 - (count - 1)

        def body(i, _):
            base = pl.multiple_of(starts[c] + i * few, few)
            total = None
            for r in range(8):
                part = None
                tall = few if r == 0 else few + 8
                for q in range(5):
                    k = 8 * q + r - lead
                    if 0 <= k < count:
                        term = glu[pl.ds(base + 8 * q, tall)] * tapf[pl.ds(k, 1)]
                        part = term if part is None else part + term
                part = part[r : r + few]
                total = part if total is None else total + part
            centre = total - jnp.mean(total, axis=-1, keepdims=True)
            spread = jnp.mean(centre * centre, axis=-1, keepdims=True)
            normal = centre * lax.rsqrt(spread + FLOOR) * headg[...].astype(F32)
            lanes = pl.ds(pl.multiple_of(core * SIDE * width + y * width, width), width)
            heads[pl.ds(base, few), lanes] = jax.nn.silu(normal).astype(BF16)
            return 0

        lax.fori_loop(0, SIZES[c] // few, body, 0)

    def hidden(c):
        at = pl.ds(starts[c], SIZES[c])
        lanes = pl.ds(pl.multiple_of(tp * cols, cols), cols)
        mine = pl.ds(pl.multiple_of(core * SIDE * cols + y * cols, cols), cols)
        weight = jnp.concatenate(
            [obuf[:, 2 * k : 2 * k + 2].reshape(SIDE * width, cols) for k in range(2)], axis=0
        )
        total = jnp.dot(heads[at], weight, preferred_element_type=F32)
        hid[at, mine] = (tok[at, lanes].astype(F32) + total).astype(BF16)

    def gate(c, n):
        at, lanes = pl.ds(starts[c], SIZES[c]), pl.ds(n * step, step)
        weight = fgbuf[:, :, :, :, lanes].reshape(model, step)
        ffg[pl.ds(8 + starts[c], SIZES[c]), lanes] = jnp.dot(nb[at], weight, preferred_element_type=F32)
        few = 32
        for i in range(SIZES[c] // few):
            base = starts[c] + i * few
            seen = ffg[pl.ds(base, few + 8), lanes]
            total = seen[6 : 6 + few] * fftapf[pl.ds(0, 1), lanes]
            total = total + seen[7 : 7 + few] * fftapf[pl.ds(1, 1), lanes]
            total = total + seen[8 : 8 + few] * fftapf[pl.ds(2, 1), lanes]
            act[pl.ds(base, few), lanes] = jax.nn.silu(total)

    def up(d, n):
        at = pl.ds(pl.multiple_of(around(y, d) * rows, rows), rows)
        lanes = pl.ds(n * step, step)
        weight = fubuf[:, :, :, :, lanes].reshape(model, step)
        wide = jnp.dot(nb[at], weight, preferred_element_type=F32)
        prod[core, at, lanes] = (act[at, lanes] * wide).astype(BF16)
        if n == units // step - 1:
            relay(("prod", d), prod.at[core, at], partner)

    def up_in(d):
        net.got(("prod", d))

    offsets = (0, -1, 1, 2)
    half = rows // 2

    def down(b, d):
        zb, xb = around(z, offsets[b]), around(x, offsets[b])
        at = pl.ds(pl.multiple_of(around(y, d) * rows, rows), rows)
        total = None
        for k in range(2):
            weight = jnp.concatenate(
                [
                    dbuf[0, zb, :, k].reshape(SIDE * quarter, units),
                    dbuf[1, :, xb, k].reshape(SIDE * quarter, units),
                ],
                axis=0,
            )
            part = lax.dot_general(prod[k, at], weight, NT, preferred_element_type=F32)
            total = part if total is None else total + part
        return total

    def ra(b):
        ts2[b] = down(b, 2).astype(BF16)
        net.send(("r1", b, "p"), ts2.at[b, pl.ds(0, half)], r1p.at[b], yp)
        net.send(("r1", b, "m"), ts2.at[b, pl.ds(half, half)], r1m.at[b], ym)

    def rb(b):
        tf[b, 0] = down(b, 1)
        tf[b, 1] = down(b, -1)

    def rc(b):
        top, low = pl.ds(0, half), pl.ds(half, half)
        net.got(("r1", b, "p"))
        net.got(("r1", b, "m"))
        tsp[b, top] = (tf[b, 0, top] + r1p[b].astype(F32)).astype(BF16)
        tsp[b, low] = tf[b, 0, low].astype(BF16)
        net.send(("r2", b, "p"), tsp.at[b], r2p.at[b], yp)
        tsm[b, low] = (tf[b, 1, low] + r1m[b].astype(F32)).astype(BF16)
        tsm[b, top] = tf[b, 1, top].astype(BF16)
        net.send(("r2", b, "m"), tsm.at[b], r2m.at[b], ym)

    def rd(b):
        tf[b, 2] = down(b, 0)

    def re(b):
        net.got(("r2", b, "p"))
        net.got(("r2", b, "m"))
        mine = pl.ds(pl.multiple_of(core * half, half), half)
        other = pl.ds(pl.multiple_of((1 - core) * half, half), half)
        xsend[b] = tf[b, 2, other] + r2p[b, other].astype(F32) + r2m[b, other].astype(F32)
        net.send(("r3", b), xsend.at[b], xrecv.at[b], partner)
        own[b] = tf[b, 2, mine] + r2p[b, mine].astype(F32) + r2m[b, mine].astype(F32)

    def rf(b):
        zb, xb = around(z, offsets[b]), around(x, offsets[b])
        net.got(("r3", b))
        mine, other = own[b], xrecv[b]
        low = jnp.where(core == 0, mine, other)
        high = jnp.where(core == 0, other, mine)
        for j in range(SIDE):
            for u in range(2):
                at = (u * SIDE + j) * quarter
                both = jnp.concatenate([low[:, at : at + quarter], high[:, at : at + quarter]], axis=1)
                if u == 0:
                    outf[zb, j, :, pl.ds(0, 2 * quarter)] = both
                else:
                    outf[j, xb, :, pl.ds(2 * quarter, 2 * quarter)] = both

    H = ("H", heads, width)
    own_blocks = {
        "V": ("v", "g"),
        **{n: ((n, 0), (n, 1)) for n in "OGUD"},
    }
    in_order = [(t % 2) * SIDE * cols + (t // 2) * cols for t in range(8)]
    I = ("I", hid, cols)

    def ready(*keys):
        for key in keys:
            if key in local:
                local.pop(key).wait()

    def halves():
        for u in range(2):
            theirs = pl.multiple_of(u * half_f + (1 - core) * quarter, quarter)
            net.send(("d", u), down_hbm.at[pl.ds(theirs, quarter)], dbuf.at[u, z, x, core], partner)

    def halves_in():
        for u in range(2):
            net.got(("d", u))

    def loads():
        for c in range(SIDE):
            load(("tok", c), tok_hbm.at[0, pl.ds(c * rows, rows)], tok.at[pl.ds(c * rows, rows)])
            if c == 0:
                for u in range(2):
                    load(("O", u), out_hbm.at[pl.ds(u * half_o, half_o)], obuf.at[z, x, u])
        for u in range(2):
            load(("G", u), fg_hbm.at[pl.ds(u * half_f, half_f)], fgbuf.at[z, x, u])
            load(("U", u), fu_hbm.at[pl.ds(u * half_f, half_f)], fubuf.at[z, x, u])
            mine = pl.multiple_of(u * half_f + core * quarter, quarter)
            load(("D", u), down_hbm.at[pl.ds(mine, quarter)], dbuf.at[u, z, x, core])

    def tables():
        tapf[pl.ds(0, taps.shape[0])] = taps[...].astype(F32)
        fftapf[pl.ds(0, fftaps.shape[0])] = fftaps[...].astype(F32)
        glu[pl.ds(0, 32)] = jnp.zeros((32, glu.shape[1]), F32)
        ffg[pl.ds(0, 8)] = jnp.zeros((8, units), F32)

    def normed(c):
        ready(("tok", c))
        norm(tok, mixg, c * rows, rows, [0])

    def renormed(c):
        norm(hid, ffng, starts[c], SIZES[c], in_order)

    def meet():
        pl.semaphore_wait(barrier, len(peers))

    for step_of, *given in (
        (loads,), (meet,), (s1, "V", 0), (s1, "V", 1), (tables,), (s1, "O", 0), (s1, "O", 1), (halves,),
        (s1, "G", 0), (s1, "G", 1), (normed, 0), (normed, 1), (halves_in,), (normed, 2), (normed, 3),
        (s2, "V", 0), (s2, "V", 1), (s1, "U", 0), (s1, "U", 1), (s2, "O", 0), (s2, "O", 1), (s2, "G", 0),
        (s2, "G", 1), (s3, "V", 0), (s3, "V", 1), (s3, "O", 0), (s3, "O", 1), (s4, "V", 0), (s4, "V", 1),
        (s3, "G", 0), (s3, "G", 1), (s1, "D", 0), (s1, "D", 1), (s5, "V", 0), (s5, "V", 1), (s4, "O", 0),
        (s4, "O", 1), (s5, "O", 0), (s5, "O", 1), (s6, "V", 0), (s6, "V", 1), (s2, "U", 0), (s2, "U", 1),
        (mixa, 0), (mix, 0), (a1, *H, 0), (mixa, 1), (mix, 1), (a1, *H, 1), (mixa, 2), (mix, 2),
        (a1, *H, 2), (s4, "G", 0), (s4, "G", 1), (mixa, 3), (a2, *H, 0), (mix, 3), (a1, *H, 3), (mixa, 4),
        (mix, 4), (a1, *H, 4), (a2, *H, 1), (s5, "G", 0), (s5, "G", 1), (a2, *H, 2), (a3, *H, 0),
        (a2, *H, 3), (a4, "H", 0), (a2, *H, 4), (s6, "O", 0), (s6, "O", 1), (hidden, 0), (a1, *I, 0),
        (a3, *H, 1), (s3, "U", 0), (s3, "U", 1), (s2, "D", 0), (s2, "D", 1), (a3, *H, 2), (a4, "H", 1),
        (hidden, 1), (a1, *I, 1), (a3, *H, 3), (a4, "H", 2), (hidden, 2), (a3, *H, 4), (a4, "H", 3),
        (hidden, 3), (a4, "H", 4), (hidden, 4), (a2, *I, 0), (a1, *I, 2), (s6, "G", 0), (s6, "G", 1),
        (a2, *I, 1), (a1, *I, 3), (a3, *I, 0), (s4, "U", 0), (s4, "U", 1), (a4, "I", 0), (renormed, 0),
        (gate, 0, 0), (gate, 0, 1), (a2, *I, 2), (a1, *I, 4), (gate, 0, 2), (a3, *I, 1), (s5, "U", 0),
        (s5, "U", 1), (s3, "D", 0), (s3, "D", 1), (a4, "I", 1), (renormed, 1), (a2, *I, 3), (gate, 1, 0),
        (gate, 1, 1), (a3, *I, 2), (gate, 1, 2), (a2, *I, 4), (a4, "I", 2), (renormed, 2), (s6, "U", 0),
        (s6, "U", 1), (gate, 2, 0), (a3, *I, 3), (gate, 2, 1), (gate, 2, 2), (a4, "I", 3), (renormed, 3),
        (a3, *I, 4), (gate, 3, 0), (gate, 3, 1), (gate, 3, 2), (s4, "D", 0), (s4, "D", 1), (a4, "I", 4),
        (renormed, 4), (gate, 4, 0), (gate, 4, 1), (gate, 4, 2), (up, 2, 0), (up, 2, 1), (up, 2, 2),
        (up, 1, 0), (up, 1, 1), (up, 1, 2), (up, -1, 0), (up, -1, 1), (up_in, 2), (s5, "D", 0),
        (s5, "D", 1), (ra, 0), (ra, 1), (ra, 2), (up_in, 1), (up, -1, 2), (up, 0, 0), (up, 0, 1),
        (up, 0, 2), (up_in, -1), (rb, 0), (s6, "D", 0), (s6, "D", 1), (ra, 3), (up_in, 0), (rd, 0),
        (rc, 0), (rb, 1), (rc, 1), (rd, 1), (rb, 2), (rc, 2), (rd, 2), (rb, 3), (rc, 3), (rd, 3), (re, 0),
        (rf, 0), (re, 1), (rf, 1), (re, 2), (rf, 2), (re, 3), (rf, 3),
    ):
        tag = "_".join(str(part) for part in given if isinstance(part, (int, str)))
        with jax.named_scope(step_of.__name__ + "_" + tag):
            step_of(*given)
    positions = length // 8
    at = pl.ds(pl.multiple_of(tp * positions, positions), positions)
    with jax.named_scope("result"):
        for zi in range(SIDE):
            for xi in range(SIDE):
                lanes = pl.ds((zi * SIDE + xi) * 4 * quarter, 4 * quarter)
                start = in_order[2 * zi + xi // 2] + (xi % 2) * 4 * quarter
                total = hid[at, pl.ds(start, 4 * quarter)].astype(F32) + outf[zi, xi]
                out_ref[0, :, lanes] = total.astype(BF16)
    with jax.named_scope("drain"):
        net.drain()


def on_device(
    tokens,
    mix_gain,
    value_weight,
    gate_weight,
    mix_taps,
    head_gain,
    out_weight,
    ffn_gain,
    ffgate_weight,
    up_weight,
    ff_taps,
    down_weight,
):
    _, length, model = tokens.shape
    width, cols, units = value_weight.shape[1], out_weight.shape[1], ffgate_weight.shape[1]
    deep, deep_o, deep_d = value_weight.shape[0], out_weight.shape[0], down_weight.shape[0]
    rows, positions, part = length // SIDE, length // 8, 2 * deep_d
    vmem = pl.BlockSpec(memory_space=pltpu.VMEM)
    hbm = pl.BlockSpec(memory_space=pl.ANY)
    four = (SIDE, SIDE)
    scratch = [
        pltpu.VMEM((length, model), BF16),
        pltpu.VMEM((length, model), BF16),
        pltpu.VMEM((*four, deep, width), BF16),
        pltpu.VMEM((*four, deep, width), BF16),
        pltpu.VMEM((*four, 2, deep_o // 2, cols), BF16),
        pltpu.VMEM((*four, 2, deep // 2, units), BF16),
        pltpu.VMEM((*four, 2, deep // 2, units), BF16),
        pltpu.VMEM((2, *four, 2, deep_d // 4, units), BF16),
        pltpu.VMEM((32, width), F32),
        pltpu.VMEM((8, units), F32),
        pltpu.VMEM((32 + length, width), F32),
        pltpu.VMEM((length, 8 * width), BF16),
        pltpu.VMEM((length, 8 * cols), BF16),
        pltpu.VMEM((8 + length, units), F32),
        pltpu.VMEM((length, units), F32),
        pltpu.VMEM((2, length, units), BF16),
        pltpu.VMEM((4, rows, part), BF16),
        pltpu.VMEM((4, rows, part), BF16),
        pltpu.VMEM((4, rows, part), BF16),
        pltpu.VMEM((4, 3, rows, part), F32),
        pltpu.VMEM((4, rows // 2, part), BF16),
        pltpu.VMEM((4, rows // 2, part), BF16),
        pltpu.VMEM((4, rows, part), BF16),
        pltpu.VMEM((4, rows, part), BF16),
        pltpu.VMEM((4, rows // 2, part), F32),
        pltpu.VMEM((4, rows // 2, part), F32),
        pltpu.VMEM((4, rows // 2, part), F32),
        pltpu.VMEM((*four, positions, deep_d), F32),
        pltpu.SemaphoreType.DMA((POOL,)),
        pltpu.SemaphoreType.DMA((RECEIVES,)),
        pltpu.SemaphoreType.DMA((14,)),
    ]
    return pl.pallas_call(
        kernel,
        out_shape=jax.ShapeDtypeStruct((1, positions, model), BF16),
        in_specs=[hbm, vmem, hbm, hbm, vmem, vmem, hbm, vmem, hbm, hbm, vmem, hbm],
        out_specs=vmem,
        scratch_shapes=scratch,
        compiler_params=pltpu.CompilerParams(
            collective_id=0, has_side_effects=True, vmem_limit_bytes=60 * 1024 * 1024
        ),
        name="layer",
    )(
        tokens,
        mix_gain,
        value_weight,
        gate_weight,
        mix_taps,
        head_gain.reshape(1, -1),
        out_weight,
        ffn_gain,
        ffgate_weight,
        up_weight,
        ff_taps,
        down_weight,
    )


def solution(mesh):
    placed = (
        P(("rep", "fs"), None, None),
        P(),
        P("fs", "tp"),
        P("fs", "tp"),
        P(None, "tp"),
        P("tp"),
        P("fs", "tp"),
        P(),
        P("fs", "tp"),
        P("fs", "tp"),
        P(None, "tp"),
        P("fs", "tp"),
    )
    return jax.shard_map(
        on_device,
        mesh=mesh,
        in_specs=placed,
        out_specs=P(("rep", "fs"), "tp", None),
        check_vma=False,
    )
```

```python
import jax
import jax.numpy as jnp
from jax import lax
from jax.experimental import pallas as pl
from jax.experimental.pallas import tpu as pltpu
from jax.sharding import PartitionSpec as P

FLOOR = 0.01
SIZES = (192, 256, 256, 192, 128)
SIDE = 4
F32 = jnp.float32
BF16 = jnp.bfloat16
NT = (((1,), (1,)), ((), ()))


SETS = {"V": "x", "U": "x", "O": "y", "D": "y", "G": "z"}
RING = {"H": 1, "I": 1, "r1": 1, "r2": 1}
FAR = {"p": "pp", "m": "mm"}
POOL = 56
RECEIVES = 116


def slot_of(key):
    name = key[0]
    if name in SETS:
        return (SETS[name] if key[2] > 2 else name, *key[1:])
    if name in RING and key[2] != "c":
        return ("ring", key[1], FAR[key[2]] if name == "r2" else key[2])
    return key


class Exchange:
    def __init__(self, send_sems, recv_sems):
        self.send_sems, self.recv_sems, self.copies, self.slots = send_sems, recv_sems, {}, {}
        self.started = []

    def send(self, key, src, dst, device):
        turn = len(self.started)
        if turn >= POOL:
            self.started[turn - POOL].wait_send()
        at = self.slots.setdefault(slot_of(key), len(self.slots))
        copy = pltpu.make_async_remote_copy(
            src_ref=src,
            dst_ref=dst,
            send_sem=self.send_sems.at[turn % POOL],
            recv_sem=self.recv_sems.at[at],
            device_id=device,
            device_id_type=pl.DeviceIdType.MESH,
        )
        copy.start()
        self.started.append(copy)
        self.copies[key] = copy

    def got(self, key):
        self.copies[key].wait_recv()

    def drain(self):
        assert len(self.slots) == RECEIVES, len(self.slots)
        for copy in self.started[-POOL:]:
            copy.wait_send()


def kernel(
    tok_hbm, mixg, value_hbm, gate_hbm, taps, headg, out_hbm, ffng,
    fg_hbm, fu_hbm, fftaps, down_hbm,
    out_ref,
    tok, nb, vbuf, gbuf, obuf, fgbuf, fubuf, dbuf,
    tapf, fftapf, glu, heads, hid, ffg, act, prod,
    ts2, tsp, tsm, tf, r1p, r1m, r2p, r2m, xsend, xrecv, own, outf,
    send_sems, recv_sems, local_sems,
):
    length = nb.shape[0]
    rows = length // SIDE
    starts = [sum(SIZES[:c]) for c in range(len(SIZES))]
    model = nb.shape[1]
    width = heads.shape[1] // 8
    cols = hid.shape[1] // 8
    units = ffg.shape[1]
    step = 256

    rep, fs, tp = lax.axis_index("rep"), lax.axis_index("fs"), lax.axis_index("tp")
    z, x = lax.div(fs, SIDE), lax.rem(fs, SIDE)
    y, core = lax.div(tp, 2), lax.rem(tp, 2)

    def around(i, d):
        return lax.rem(i + d + SIDE, SIDE)

    def along_x(d):
        return (rep, z * SIDE + around(x, d), tp)

    def along_z(d):
        at = lax.rem(rep * SIDE + z + d + 2 * SIDE, 2 * SIDE)
        return (lax.div(at, SIDE), lax.rem(at, SIDE) * SIDE + x, tp)

    def along_y(d):
        return (rep, fs, around(y, d) * 2 + core)

    partner = (rep, fs, y * 2 + 1 - core)
    yp, ym = along_y(1), along_y(-1)
    x_ring, z_ring = (along_x(1), along_x(-1)), (along_z(1), along_z(-1))
    first_ring, second_ring = (x_ring, z_ring), (z_ring, x_ring)
    place = (z, x)

    barrier = pltpu.get_barrier_semaphore()
    peers = (*x_ring, *z_ring, yp, ym, partner)
    for peer in peers:
        pl.semaphore_signal(barrier, inc=1, device_id=peer, device_id_type=pl.DeviceIdType.MESH)

    local = {}

    def load(key, src, dst):
        copy = pltpu.make_async_copy(src, dst, local_sems.at[len(local)])
        copy.start()
        local[key] = copy

    load("v", value_hbm, vbuf.at[z, x])
    load("g", gate_hbm, gbuf.at[z, x])
    half_o, half_f = out_hbm.shape[0] // 2, fg_hbm.shape[0] // 2
    quarter = down_hbm.shape[0] // 4
    net = Exchange(send_sems, recv_sems)

    def pick_v(u, zi, xi, h=None):
        ref = (vbuf, gbuf)[u]
        half = value_hbm.shape[0] // 2
        return ref.at[zi, xi] if h is None else ref.at[zi, xi, pl.ds(h * half, half)]

    def pick_of(ref):
        def pick(u, zi, xi, h=None):
            half = ref.shape[3] // 2
            return ref.at[zi, xi, u] if h is None else ref.at[zi, xi, u, pl.ds(h * half, half)]

        return pick

    def pick_d(u, zi, xi, h=None):
        return dbuf.at[u, zi, xi] if h is None else dbuf.at[u, zi, xi, h]

    picks = {"V": pick_v, "O": pick_of(obuf), "G": pick_of(fgbuf), "U": pick_of(fubuf), "D": pick_d}

    def near(n, u, d, h=None):
        if u == 0:
            return picks[n](0, z, around(x, d), h)
        return picks[n](1, around(z, d), x, h)

    def block(n, u, d, h):
        pair = pl.ds(2 * h, 2)
        if u == 0:
            return picks[n](0, around(z, d), pair)
        return picks[n](1, pair, around(x, d))

    def relay(key, ref, device):
        net.send(key, ref, ref, device)

    def s1(n, u):
        if u == 0 or n in "V":
            ready(*own_blocks[n])
        ref = picks[n](u, z, x)
        relay((n, u, 1, "p"), ref, first_ring[u][0])
        relay((n, u, 1, "m"), ref, first_ring[u][1])

    def s2(n, u):
        net.got((n, u, 1, "p"))
        net.got((n, u, 1, "m"))
        relay((n, u, 2, "p"), near(n, u, -1, 0), first_ring[u][0])
        relay((n, u, 2, "m"), near(n, u, 1, 1), first_ring[u][1])

    def s3(n, u):
        for v in {"U": (0, 1), "D": (0, 1)}.get(n, (u,)) if u == 0 or n not in "UD" else ():
            net.got((n, v, 2, "p"))
            net.got((n, v, 2, "m"))
        plus, minus = second_ring[u]
        relay((n, u, 3, "p0"), block(n, u, 0, 0), plus)
        relay((n, u, 3, "m0"), block(n, u, 0, 1), minus)
        relay((n, u, 3, "p1"), block(n, u, 0, 1), plus)
        relay((n, u, 3, "m1"), block(n, u, 0, 0), minus)

    def s4(n, u):
        plus, minus = second_ring[u]
        net.got((n, u, 3, "p0"))
        relay((n, u, 4, "p"), block(n, u, -1, 0), plus)
        net.got((n, u, 3, "m0"))
        relay((n, u, 4, "m"), block(n, u, 1, 1), minus)

    def s5(n, u):
        net.got((n, u, 3, "p1"))
        net.got((n, u, 3, "m1"))

    def s6(n, u):
        net.got((n, u, 4, "p"))
        net.got((n, u, 4, "m"))

    def chunk_ref(buf, wide, c, d, h=None):
        count = SIZES[c] if h is None else SIZES[c] // 2
        start = starts[c] + (0 if h is None else h * count)
        lane = pl.multiple_of(core * SIDE * wide + around(y, d) * wide, wide)
        return buf.at[pl.ds(start, count), pl.ds(lane, wide)]

    def a1(n, buf, wide, c):
        ref = chunk_ref(buf, wide, c, 0)
        relay((n, c, "p"), ref, yp)
        relay((n, c, "m"), ref, ym)

    def a2(n, buf, wide, c):
        net.got((n, c, "p"))
        net.got((n, c, "m"))
        relay((n, c, "pp"), chunk_ref(buf, wide, c, -1, h=0), yp)
        relay((n, c, "mm"), chunk_ref(buf, wide, c, 1, h=1), ym)

    def a3(n, buf, wide, c):
        net.got((n, c, "pp"))
        net.got((n, c, "mm"))
        lane = pl.multiple_of(core * SIDE * wide, SIDE * wide)
        relay((n, c, "c"), buf.at[pl.ds(starts[c], SIZES[c]), pl.ds(lane, SIDE * wide)], partner)

    def a4(n, c):
        net.got((n, c, "c"))

    def norm(src, gain, first, count, lanes):
        few, wide = 16, model // len(lanes)

        def body(i, _):
            at = pl.ds(pl.multiple_of(first + i * few, few), few)
            parts = [src[at, pl.ds(start, wide)] for start in lanes]
            value = jnp.concatenate(parts, axis=1).astype(F32)
            scale = lax.rsqrt(jnp.mean(value * value, axis=-1, keepdims=True) + FLOOR)
            nb[at] = (value * scale * gain[...].astype(F32).reshape(1, model)).astype(BF16)
            return 0

        lax.fori_loop(0, count // few, body, 0, unroll=4)

    def mixa(c):
        at = pl.ds(starts[c], SIZES[c])
        both = jnp.concatenate(
            [vbuf[...].reshape(model, width), gbuf[...].reshape(model, width)], axis=1
        )
        pair = jnp.dot(nb[at], both, preferred_element_type=F32)
        glu[pl.ds(32 + starts[c], SIZES[c])] = pair[:, :width] * jax.nn.sigmoid(pair[:, width:])

    def mix(c):
        few, count = 64, taps.shape[0]
        lead = 32 - (count - 1)

        def body(i, _):
            base = pl.multiple_of(starts[c] + i * few, few)
            total = None
            for r in range(8):
                part = None
                tall = few if r == 0 else few + 8
                for q in range(5):
                    k = 8 * q + r - lead
                    if 0 <= k < count:
                        term = glu[pl.ds(base + 8 * q, tall)] * tapf[pl.ds(k, 1)]
                        part = term if part is None else part + term
                part = part[r : r + few]
                total = part if total is None else total + part
            centre = total - jnp.mean(total, axis=-1, keepdims=True)
            spread = jnp.mean(centre * centre, axis=-1, keepdims=True)
            normal = centre * lax.rsqrt(spread + FLOOR) * headg[...].astype(F32)
            lanes = pl.ds(pl.multiple_of(core * SIDE * width + y * width, width), width)
            heads[pl.ds(base, few), lanes] = jax.nn.silu(normal).astype(BF16)
            return 0

        lax.fori_loop(0, SIZES[c] // few, body, 0)

    def hidden(c):
        at = pl.ds(starts[c], SIZES[c])
        lanes = pl.ds(pl.multiple_of(tp * cols, cols), cols)
        mine = pl.ds(pl.multiple_of(core * SIDE * cols + y * cols, cols), cols)
        weight = jnp.concatenate(
            [obuf[:, 2 * k : 2 * k + 2].reshape(SIDE * width, cols) for k in range(2)], axis=0
        )
        total = jnp.dot(heads[at], weight, preferred_element_type=F32)
        hid[at, mine] = (tok[at, lanes].astype(F32) + total).astype(BF16)

    def gate(c, n):
        at, lanes = pl.ds(starts[c], SIZES[c]), pl.ds(n * step, step)
        weight = fgbuf[:, :, :, :, lanes].reshape(model, step)
        ffg[pl.ds(8 + starts[c], SIZES[c]), lanes] = jnp.dot(nb[at], weight, preferred_element_type=F32)
        few = 32
        for i in range(SIZES[c] // few):
            base = starts[c] + i * few
            seen = ffg[pl.ds(base, few + 8), lanes]
            total = seen[6 : 6 + few] * fftapf[pl.ds(0, 1), lanes]
            total = total + seen[7 : 7 + few] * fftapf[pl.ds(1, 1), lanes]
            total = total + seen[8 : 8 + few] * fftapf[pl.ds(2, 1), lanes]
            act[pl.ds(base, few), lanes] = jax.nn.silu(total)

    def up(d, n):
        at = pl.ds(pl.multiple_of(around(y, d) * rows, rows), rows)
        lanes = pl.ds(n * step, step)
        weight = fubuf[:, :, :, :, lanes].reshape(model, step)
        wide = jnp.dot(nb[at], weight, preferred_element_type=F32)
        prod[core, at, lanes] = (act[at, lanes] * wide).astype(BF16)
        if n == units // step - 1:
            relay(("prod", d), prod.at[core, at], partner)

    def up_in(d):
        net.got(("prod", d))

    offsets = (0, -1, 1, 2)
    half = rows // 2

    def down(b, d):
        zb, xb = around(z, offsets[b]), around(x, offsets[b])
        at = pl.ds(pl.multiple_of(around(y, d) * rows, rows), rows)
        total = None
        for k in range(2):
            weight = jnp.concatenate(
                [
                    dbuf[0, zb, :, k].reshape(SIDE * quarter, units),
                    dbuf[1, :, xb, k].reshape(SIDE * quarter, units),
                ],
                axis=0,
            )
            part = lax.dot_general(prod[k, at], weight, NT, preferred_element_type=F32)
            total = part if total is None else total + part
        return total

    def ra(b):
        ts2[b] = down(b, 2).astype(BF16)
        net.send(("r1", b, "p"), ts2.at[b, pl.ds(0, half)], r1p.at[b], yp)
        net.send(("r1", b, "m"), ts2.at[b, pl.ds(half, half)], r1m.at[b], ym)

    def rb(b):
        tf[b, 0] = down(b, 1)
        tf[b, 1] = down(b, -1)

    def rc(b):
        top, low = pl.ds(0, half), pl.ds(half, half)
        net.got(("r1", b, "p"))
        net.got(("r1", b, "m"))
        tsp[b, top] = (tf[b, 0, top] + r1p[b].astype(F32)).astype(BF16)
        tsp[b, low] = tf[b, 0, low].astype(BF16)
        net.send(("r2", b, "p"), tsp.at[b], r2p.at[b], yp)
        tsm[b, low] = (tf[b, 1, low] + r1m[b].astype(F32)).astype(BF16)
        tsm[b, top] = tf[b, 1, top].astype(BF16)
        net.send(("r2", b, "m"), tsm.at[b], r2m.at[b], ym)

    def rd(b):
        tf[b, 2] = down(b, 0)

    def re(b):
        net.got(("r2", b, "p"))
        net.got(("r2", b, "m"))
        mine = pl.ds(pl.multiple_of(core * half, half), half)
        other = pl.ds(pl.multiple_of((1 - core) * half, half), half)
        xsend[b] = tf[b, 2, other] + r2p[b, other].astype(F32) + r2m[b, other].astype(F32)
        net.send(("r3", b), xsend.at[b], xrecv.at[b], partner)
        own[b] = tf[b, 2, mine] + r2p[b, mine].astype(F32) + r2m[b, mine].astype(F32)

    def rf(b):
        zb, xb = around(z, offsets[b]), around(x, offsets[b])
        net.got(("r3", b))
        mine, other = own[b], xrecv[b]
        low = jnp.where(core == 0, mine, other)
        high = jnp.where(core == 0, other, mine)
        for j in range(SIDE):
            for u in range(2):
                at = (u * SIDE + j) * quarter
                both = jnp.concatenate([low[:, at : at + quarter], high[:, at : at + quarter]], axis=1)
                if u == 0:
                    outf[zb, j, :, pl.ds(0, 2 * quarter)] = both
                else:
                    outf[j, xb, :, pl.ds(2 * quarter, 2 * quarter)] = both

    H = ("H", heads, width)
    own_blocks = {
        "V": ("v", "g"),
        **{n: ((n, 0), (n, 1)) for n in "OGUD"},
    }
    in_order = [(t % 2) * SIDE * cols + (t // 2) * cols for t in range(8)]
    I = ("I", hid, cols)

    def ready(*keys):
        for key in keys:
            if key in local:
                local.pop(key).wait()

    def halves():
        for u in range(2):
            theirs = pl.multiple_of(u * half_f + (1 - core) * quarter, quarter)
            net.send(("d", u), down_hbm.at[pl.ds(theirs, quarter)], dbuf.at[u, z, x, core], partner)

    def halves_in():
        for u in range(2):
            net.got(("d", u))

    def loads():
        for c in range(SIDE):
            load(("tok", c), tok_hbm.at[0, pl.ds(c * rows, rows)], tok.at[pl.ds(c * rows, rows)])
            if c == 0:
                for u in range(2):
                    load(("O", u), out_hbm.at[pl.ds(u * half_o, half_o)], obuf.at[z, x, u])
        for u in range(2):
            load(("G", u), fg_hbm.at[pl.ds(u * half_f, half_f)], fgbuf.at[z, x, u])
            load(("U", u), fu_hbm.at[pl.ds(u * half_f, half_f)], fubuf.at[z, x, u])
            mine = pl.multiple_of(u * half_f + core * quarter, quarter)
            load(("D", u), down_hbm.at[pl.ds(mine, quarter)], dbuf.at[u, z, x, core])

    def tables():
        tapf[pl.ds(0, taps.shape[0])] = taps[...].astype(F32)
        fftapf[pl.ds(0, fftaps.shape[0])] = fftaps[...].astype(F32)
        glu[pl.ds(0, 32)] = jnp.zeros((32, glu.shape[1]), F32)
        ffg[pl.ds(0, 8)] = jnp.zeros((8, units), F32)

    def normed(c):
        ready(("tok", c))
        norm(tok, mixg, c * rows, rows, [0])

    def renormed(c):
        norm(hid, ffng, starts[c], SIZES[c], in_order)

    def meet():
        pl.semaphore_wait(barrier, len(peers))

    for step_of, *given in (
        (loads,), (meet,), (s1, "V", 0), (s1, "V", 1), (tables,), (s1, "O", 0), (s1, "O", 1), (halves,),
        (s1, "G", 0), (s1, "G", 1), (normed, 0), (normed, 1), (halves_in,), (normed, 2), (normed, 3),
        (s2, "V", 0), (s2, "V", 1), (s1, "U", 0), (s1, "U", 1), (s2, "O", 0), (s2, "O", 1), (s2, "G", 0),
        (s2, "G", 1), (s3, "V", 0), (s3, "V", 1), (s3, "O", 0), (s3, "O", 1), (s4, "V", 0), (s4, "V", 1),
        (s3, "G", 0), (s3, "G", 1), (s1, "D", 0), (s1, "D", 1), (s5, "V", 0), (s5, "V", 1), (s4, "O", 0),
        (s4, "O", 1), (s5, "O", 0), (s5, "O", 1), (s6, "V", 0), (s6, "V", 1), (s2, "U", 0), (s2, "U", 1),
        (mixa, 0), (mix, 0), (a1, *H, 0), (mixa, 1), (mix, 1), (a1, *H, 1), (mixa, 2), (mix, 2),
        (a1, *H, 2), (s4, "G", 0), (s4, "G", 1), (mixa, 3), (a2, *H, 0), (mix, 3), (a1, *H, 3), (mixa, 4),
        (mix, 4), (a1, *H, 4), (a2, *H, 1), (s5, "G", 0), (s5, "G", 1), (a2, *H, 2), (a3, *H, 0),
        (a2, *H, 3), (a4, "H", 0), (a2, *H, 4), (s6, "O", 0), (s6, "O", 1), (hidden, 0), (a1, *I, 0),
        (a3, *H, 1), (s3, "U", 0), (s3, "U", 1), (s2, "D", 0), (s2, "D", 1), (a3, *H, 2), (a4, "H", 1),
        (hidden, 1), (a1, *I, 1), (a3, *H, 3), (a4, "H", 2), (hidden, 2), (a3, *H, 4), (a4, "H", 3),
        (hidden, 3), (a4, "H", 4), (hidden, 4), (a2, *I, 0), (a1, *I, 2), (s6, "G", 0), (s6, "G", 1),
        (a2, *I, 1), (a1, *I, 3), (a3, *I, 0), (s4, "U", 0), (s4, "U", 1), (a4, "I", 0), (renormed, 0),
        (gate, 0, 0), (gate, 0, 1), (a2, *I, 2), (a1, *I, 4), (gate, 0, 2), (a3, *I, 1), (s5, "U", 0),
        (s5, "U", 1), (s3, "D", 0), (s3, "D", 1), (a4, "I", 1), (renormed, 1), (a2, *I, 3), (gate, 1, 0),
        (gate, 1, 1), (a3, *I, 2), (gate, 1, 2), (a2, *I, 4), (a4, "I", 2), (renormed, 2), (s6, "U", 0),
        (s6, "U", 1), (gate, 2, 0), (a3, *I, 3), (gate, 2, 1), (gate, 2, 2), (a4, "I", 3), (renormed, 3),
        (a3, *I, 4), (gate, 3, 0), (gate, 3, 1), (gate, 3, 2), (s4, "D", 0), (s4, "D", 1), (a4, "I", 4),
        (renormed, 4), (gate, 4, 0), (gate, 4, 1), (gate, 4, 2), (up, 2, 0), (up, 2, 1), (up, 2, 2),
        (up, 1, 0), (up, 1, 1), (up, 1, 2), (up, -1, 0), (up, -1, 1), (up_in, 2), (s5, "D", 0),
        (s5, "D", 1), (ra, 0), (ra, 1), (ra, 2), (up_in, 1), (up, -1, 2), (up, 0, 0), (up, 0, 1),
        (up, 0, 2), (up_in, -1), (rb, 0), (s6, "D", 0), (s6, "D", 1), (ra, 3), (up_in, 0), (rd, 0),
        (rc, 0), (rb, 1), (rc, 1), (rd, 1), (rb, 2), (rc, 2), (rd, 2), (rb, 3), (rc, 3), (rd, 3), (re, 0),
        (rf, 0), (re, 1), (rf, 1), (re, 2), (rf, 2), (re, 3), (rf, 3),
    ):
        tag = "_".join(str(part) for part in given if isinstance(part, (int, str)))
        with jax.named_scope(step_of.__name__ + "_" + tag):
            step_of(*given)
    positions = length // 8
    at = pl.ds(pl.multiple_of(tp * positions, positions), positions)
    with jax.named_scope("result"):
        for zi in range(SIDE):
            for xi in range(SIDE):
                lanes = pl.ds((zi * SIDE + xi) * 4 * quarter, 4 * quarter)
                start = in_order[2 * zi + xi // 2] + (xi % 2) * 4 * quarter
                total = hid[at, pl.ds(start, 4 * quarter)].astype(F32) + outf[zi, xi]
                out_ref[0, :, lanes] = total.astype(BF16)
    with jax.named_scope("drain"):
        net.drain()


def on_device(
    tokens,
    mix_gain,
    value_weight,
    gate_weight,
    mix_taps,
    head_gain,
    out_weight,
    ffn_gain,
    ffgate_weight,
    up_weight,
    ff_taps,
    down_weight,
):
    _, length, model = tokens.shape
    width, cols, units = value_weight.shape[1], out_weight.shape[1], ffgate_weight.shape[1]
    deep, deep_o, deep_d = value_weight.shape[0], out_weight.shape[0], down_weight.shape[0]
    rows, positions, part = length // SIDE, length // 8, 2 * deep_d
    vmem = pl.BlockSpec(memory_space=pltpu.VMEM)
    hbm = pl.BlockSpec(memory_space=pl.ANY)
    four = (SIDE, SIDE)
    scratch = [
        pltpu.VMEM((length, model), BF16),
        pltpu.VMEM((length, model), BF16),
        pltpu.VMEM((*four, deep, width), BF16),
        pltpu.VMEM((*four, deep, width), BF16),
        pltpu.VMEM((*four, 2, deep_o // 2, cols), BF16),
        pltpu.VMEM((*four, 2, deep // 2, units), BF16),
        pltpu.VMEM((*four, 2, deep // 2, units), BF16),
        pltpu.VMEM((2, *four, 2, deep_d // 4, units), BF16),
        pltpu.VMEM((32, width), F32),
        pltpu.VMEM((8, units), F32),
        pltpu.VMEM((32 + length, width), F32),
        pltpu.VMEM((length, 8 * width), BF16),
        pltpu.VMEM((length, 8 * cols), BF16),
        pltpu.VMEM((8 + length, units), F32),
        pltpu.VMEM((length, units), F32),
        pltpu.VMEM((2, length, units), BF16),
        pltpu.VMEM((4, rows, part), BF16),
        pltpu.VMEM((4, rows, part), BF16),
        pltpu.VMEM((4, rows, part), BF16),
        pltpu.VMEM((4, 3, rows, part), F32),
        pltpu.VMEM((4, rows // 2, part), BF16),
        pltpu.VMEM((4, rows // 2, part), BF16),
        pltpu.VMEM((4, rows, part), BF16),
        pltpu.VMEM((4, rows, part), BF16),
        pltpu.VMEM((4, rows // 2, part), F32),
        pltpu.VMEM((4, rows // 2, part), F32),
        pltpu.VMEM((4, rows // 2, part), F32),
        pltpu.VMEM((*four, positions, deep_d), F32),
        pltpu.SemaphoreType.DMA((POOL,)),
        pltpu.SemaphoreType.DMA((RECEIVES,)),
        pltpu.SemaphoreType.DMA((14,)),
    ]
    return pl.pallas_call(
        kernel,
        out_shape=jax.ShapeDtypeStruct((1, positions, model), BF16),
        in_specs=[hbm, vmem, hbm, hbm, vmem, vmem, hbm, vmem, hbm, hbm, vmem, hbm],
        out_specs=vmem,
        scratch_shapes=scratch,
        compiler_params=pltpu.CompilerParams(
            collective_id=0, has_side_effects=True, vmem_limit_bytes=60 * 1024 * 1024
        ),
        name="layer",
    )(
        tokens,
        mix_gain,
        value_weight,
        gate_weight,
        mix_taps,
        head_gain.reshape(1, -1),
        out_weight,
        ffn_gain,
        ffgate_weight,
        up_weight,
        ff_taps,
        down_weight,
    )


def solution(mesh):
    placed = (
        P(("rep", "fs"), None, None),
        P(),
        P("fs", "tp"),
        P("fs", "tp"),
        P(None, "tp"),
        P("tp"),
        P("fs", "tp"),
        P(),
        P("fs", "tp"),
        P("fs", "tp"),
        P(None, "tp"),
        P("fs", "tp"),
    )
    return jax.shard_map(
        on_device,
        mesh=mesh,
        in_specs=placed,
        out_specs=P(("rep", "fs"), "tp", None),
        check_vma=False,
    )
```
